32 devices in a mesh: grp: 2 (over y), ep: 8 (over z, x), tp: 2 (over core).
Axes of the slice: x: 2, y: 2, z: 4, core: 2. Of those that a mesh axis runs over, the one named last changes fastest.
Arguments:
- fresh_inputs: bfloat16 [256, 2048], P(('grp', 'ep')), parts along dimension 0, may hold values from -6 to 6
- memory_arrays: float32 [256, 32, 64, 64], P(('grp', 'ep'), 'tp'), parts along dimension 0, may hold values from -4 to 4
- chosen_specialist: int32 [256, 2], P(('grp', 'ep')), parts along dimension 0, may hold values from 0 to 3, all different within a row; in each aligned block of 128 rows (0 to 127, 128 to 255, ...) at most 96 rows name the same one
- chosen_coefficient: bfloat16 [256, 2], P(('grp', 'ep')), parts along dimension 0, may hold values from 0.25 to 1
- first_rescale: float32 [2048], replicated, may hold values from 0.1 to 1.9
- second_rescale: float32 [2048], replicated, may hold values from 0.1 to 1.9
- receiver_projector: bfloat16 [2048, 2048], P('tp', 'ep'), may hold values from -0.125 to 0.125
- address_projector: bfloat16 [2048, 2048], P('tp', 'ep'), may hold values from -0.125 to 0.125
- content_projector: bfloat16 [2048, 2048], P('tp', 'ep'), may hold values from -0.125 to 0.125
- final_projector: bfloat16 [2048, 2048], P('tp', 'ep'), may hold values from -0.125 to 0.125
- forget_narrowing: bfloat16 [2048, 64], replicated, may hold values from -0.125 to 0.125
- forget_widening: bfloat16 [64, 2048], P(None, 'tp'), may hold values from -0.75 to 0.75
- forget_bias: float32 [2048], P('tp'), may hold values from -3 to 1
- learning_narrowing: bfloat16 [2048, 64], replicated, may hold values from -0.125 to 0.125
- learning_widening: bfloat16 [64, 2048], P(None, 'tp'), may hold values from -0.75 to 0.75
- learning_bias: float32 [2048], P('tp'), may hold values from -1.5 to 1.5
- lane_scaling: float32 [2048], P('tp'), may hold values from 0.1 to 1.9
- instant_reward: float32 [32, 64], P('tp'), may hold values from -0.5 to 0.5
- specialist_switch: bfloat16 [2048, 28672], P(None, ('ep', 'tp')), may hold values from -0.125 to 0.125
- specialist_expand: bfloat16 [2048, 28672], P(None, ('ep', 'tp')), may hold values from -0.125 to 0.125
- specialist_contract: bfloat16 [28672, 2048], P(('ep', 'tp')), may hold values from -0.0625 to 0.0625
- common_activator: bfloat16 [2048, 5632], P(None, ('ep', 'tp')), may hold values from -0.125 to 0.125
- common_expand: bfloat16 [2048, 5632], P(None, ('ep', 'tp')), may hold values from -0.125 to 0.125
- common_contract: bfloat16 [5632, 2048], P(('ep', 'tp')), may hold values from -0.078125 to 0.078125
- common_switch: bfloat16 [2048], replicated, may hold values from -0.125 to 0.125
Outputs:
- new_tokens: bfloat16 [256, 2048], P(('grp', 'ep', 'tp')), parts along dimension 0
- memory_after: float32 [256, 32, 64, 64], P(('grp', 'ep'), 'tp'), parts along dimension 0
The draws below stay inside these ranges and needn't reach their ends.
There are 2 independent parts, one for each index of `grp`. The reference program is written for one: setup_inputs(seed, part) draws one part's arguments, and reference() takes and returns one part's arrays. A program takes and returns all parts, laid end to end along the dimension named above; an argument that names none is the same for every part. Nothing has to cross between parts.
Inputs may be any that keep to these rules, and one draw needn't show every extreme that they name: `chosen_specialist`: each row names 2 different experts. Over the whole batch no expert is named by more than 96 rows, and in every draw some expert is named by exactly 96 rows.
All inputs are finite; a program needn't handle non-finite values.
Results may differ from the reference program's by a relative error of at most 0.014.
Values may be sent and summed in bfloat16 or wider, within the bound.
A program may use at most 128 MiB of HBM per device.

```python
import math
import jax
import jax.numpy as jnp
import numpy as np
from jax import lax

MODEL_DIM = 2048
LANE_WIDTH = 64
LANE_COUNT = 32
LOWRANK_DIM = 64
EXPERTS = 4
TOP_K = 2
FF_E = 7168
DENSE_FF = 5632
BATCH = 128
CAP = 96
N_TP = 2


def block_levels(rng, shape, pieces, low, largest):
    level, own = 1.0, jax.random.fold_in(rng, 6)
    for dim, parts in pieces:
        steps = jnp.exp(jax.random.uniform(jax.random.fold_in(own, dim), (parts,), jnp.float32, low / len(pieces), largest / len(pieces)))
        level = level * jnp.repeat(steps, shape[dim] // parts).reshape([-1 if axis == dim else 1 for axis in range(len(shape))])
    return level


def assign_block(stream_key, own, number, rows, amount, top, most, lean):
    ranking = jax.random.permutation(stream_key, amount)
    packed, common = shares(amount, rows * top, most, lean, True), shares(amount, rows * top, most, lean, False)
    places = jnp.arange(amount)

    def named(tallies, offset_by):
        used = int((tallies > 0).sum())
        fixed = max(1, used // 4)
        moved = fixed + (places - fixed + offset_by * (used - fixed)) % max(1, amount - fixed)
        return jnp.zeros((amount,), jnp.int32).at[ranking[jnp.where(places < fixed, places, moved)]].set(jnp.asarray(tallies, jnp.int32))

    tallies = jnp.where(number % 4 == 0, named(packed, number // 4), named(common, number - number // 4 - 1))
    mixed = jax.random.permutation(jax.random.fold_in(own, 3), amount)
    source_of, sink = mixed[0:amount // 2 * 2:2], mixed[1:amount // 2 * 2:2]
    slack = jnp.minimum(tallies[source_of] - 1, most - tallies[sink]) // 2
    slack = jnp.where((source_of == ranking[0]) | (sink == ranking[0]) | (tallies[sink] == 0), 0, jnp.maximum(slack, 0))
    moved = jax.random.randint(jax.random.fold_in(own, 4), (amount // 2,), 0, 1 << 20) % (slack + 1)
    tallies = tallies.at[source_of].add(-moved).at[sink].add(moved)
    members = jnp.searchsorted(jnp.cumsum(tallies), jnp.arange(rows * top), side="right").astype(jnp.int32)
    listing = members.reshape(top, rows).T
    listing = listing[jax.random.permutation(jax.random.fold_in(own, 1), rows)]
    offset_by = jax.random.randint(jax.random.fold_in(own, 2), (rows, 1), 0, top)
    return jnp.take_along_axis(listing, (jnp.arange(top)[None, :] + offset_by) % top, axis=1)


def shares(count, total, reach, lean, full):
    portions = [(1 << 20) // math.isqrt(rank ** lean) + 1 for rank in range(1, count + 1)]
    largest = reach if full else min(reach, max(-(-total // count), total * portions[0] // sum(portions)))
    least = 1 if total - largest >= count - 1 else 0
    holding, surplus = [largest] + [least] * (count - 1), total - largest - least * (count - 1)
    while surplus > 0:
        free = [i for i in range(1, count) if holding[i] < largest] or [i for i in range(1, count) if holding[i] < reach]
        pool, remaining = sum([portions[i] for i in free]), surplus
        for i in free:
            addition = min(reach - holding[i], max(1, remaining * portions[i] // pool), surplus)
            holding[i] = holding[i] + addition
            surplus = surplus - addition
    return np.array(holding)


def bell_draw(rng, dims, deviation, limit, cuts=(), dtype=jnp.bfloat16):
    gain = block_levels(rng, dims, cuts, -0.22, 0.18) if cuts else 1.0
    drawn = jax.random.normal(rng, dims, jnp.float32) * deviation * gain
    return jnp.minimum(jnp.maximum(drawn, -limit), limit).astype(dtype)


def setup_inputs(seed: int = 0, part: int = 0) -> dict:
    splits = jax.random.split(jax.random.key(seed), 26)
    own_keys = jax.random.split(jax.random.fold_in(splits[25], part), 26)
    fresh_inputs = bell_draw(own_keys[0], (BATCH, MODEL_DIM), 1.0, 6.0, ((0, 8),))
    memory_arrays = bell_draw(own_keys[1], (BATCH, LANE_COUNT, LANE_WIDTH, LANE_WIDTH), 0.5, 4.0, ((0, 8), (1, 2)), jnp.float32)
    chosen_specialist_keys = jax.random.split(jax.random.fold_in(own_keys[2], 1), BATCH // BATCH)
    chosen_specialist_turns = jax.random.permutation(jax.random.fold_in(own_keys[2], 3), BATCH // BATCH)
    chosen_specialist = jax.vmap(lambda own, number: assign_block(jax.random.fold_in(own_keys[2], 2), own, number, BATCH, EXPERTS, TOP_K, CAP, 2))(chosen_specialist_keys, chosen_specialist_turns).reshape((BATCH, TOP_K))
    chosen_coefficient = jnp.clip(0.25 + 0.75 * jax.random.uniform(own_keys[3], (BATCH, TOP_K), jnp.float32) ** block_levels(own_keys[3], (BATCH, TOP_K), ((0, 8),), -0.2, 0.2), 0.25, 1.0).astype(jnp.bfloat16)
    first_rescale = jnp.clip(1.0 + 0.18 * jax.random.normal(splits[4], (MODEL_DIM,), jnp.float32), 0.1, 1.9)
    second_rescale = jnp.clip(1.0 + 0.18 * jax.random.normal(splits[5], (MODEL_DIM,), jnp.float32), 0.1, 1.9)
    receiver_projector = bell_draw(splits[6], (MODEL_DIM, MODEL_DIM), MODEL_DIM ** -0.5, 0.125, ((0, 2), (1, 8)))
    address_projector = bell_draw(splits[7], (MODEL_DIM, MODEL_DIM), MODEL_DIM ** -0.5, 0.125, ((0, 2), (1, 8)))
    content_projector = bell_draw(splits[8], (MODEL_DIM, MODEL_DIM), MODEL_DIM ** -0.5, 0.125, ((0, 2), (1, 8)))
    final_projector = bell_draw(splits[9], (MODEL_DIM, MODEL_DIM), MODEL_DIM ** -0.5, 0.125, ((0, 2), (1, 8)))
    forget_narrowing = bell_draw(splits[10], (MODEL_DIM, LOWRANK_DIM), MODEL_DIM ** -0.5, 0.125)
    forget_widening = bell_draw(splits[11], (LOWRANK_DIM, MODEL_DIM), LOWRANK_DIM ** -0.5, 0.75, ((1, 2),))
    forget_bias = jnp.clip(-3.0 + 4.0 * jax.random.uniform(splits[12], (MODEL_DIM,), jnp.float32) ** block_levels(splits[12], (MODEL_DIM,), ((0, 2),), -0.2, 0.2), -3.0, 1.0)
    learning_narrowing = bell_draw(splits[13], (MODEL_DIM, LOWRANK_DIM), MODEL_DIM ** -0.5, 0.125)
    learning_widening = bell_draw(splits[14], (LOWRANK_DIM, MODEL_DIM), LOWRANK_DIM ** -0.5, 0.75, ((1, 2),))
    learning_bias = jnp.clip(jax.random.uniform(splits[15], (MODEL_DIM,), jnp.float32, -1.5, 1.5) * block_levels(splits[15], (MODEL_DIM,), ((0, 2),), -0.4, 0.0), -1.5, 1.5)
    lane_scaling = jnp.clip(1.0 + 0.18 * jax.random.normal(splits[16], (MODEL_DIM,), jnp.float32), 0.1, 1.9)
    instant_reward = bell_draw(splits[17], (LANE_COUNT, LANE_WIDTH), 0.1, 0.5, ((0, 2),), jnp.float32)
    specialist_switch = bell_draw(splits[18], (MODEL_DIM, EXPERTS * FF_E), MODEL_DIM ** -0.5, 0.125, ((1, 16),))
    specialist_expand = bell_draw(splits[19], (MODEL_DIM, EXPERTS * FF_E), MODEL_DIM ** -0.5, 0.125, ((1, 16),))
    specialist_contract = bell_draw(splits[20], (EXPERTS * FF_E, MODEL_DIM), FF_E ** -0.5, 0.0625, ((0, 16),))
    common_activator = bell_draw(splits[21], (MODEL_DIM, DENSE_FF), MODEL_DIM ** -0.5, 0.125, ((1, 16),))
    common_expand = bell_draw(splits[22], (MODEL_DIM, DENSE_FF), MODEL_DIM ** -0.5, 0.125, ((1, 16),))
    common_contract = bell_draw(splits[23], (DENSE_FF, MODEL_DIM), DENSE_FF ** -0.5, 0.078125, ((0, 16),))
    common_switch = bell_draw(splits[24], (MODEL_DIM,), MODEL_DIM ** -0.5, 0.125)
    return dict(fresh_inputs=fresh_inputs, memory_arrays=memory_arrays, chosen_specialist=chosen_specialist, chosen_coefficient=chosen_coefficient, first_rescale=first_rescale, second_rescale=second_rescale, receiver_projector=receiver_projector, address_projector=address_projector, content_projector=content_projector, final_projector=final_projector, forget_narrowing=forget_narrowing, forget_widening=forget_widening, forget_bias=forget_bias, learning_narrowing=learning_narrowing, learning_widening=learning_widening, learning_bias=learning_bias, lane_scaling=lane_scaling, instant_reward=instant_reward, specialist_switch=specialist_switch, specialist_expand=specialist_expand, specialist_contract=specialist_contract, common_activator=common_activator, common_expand=common_expand, common_contract=common_contract, common_switch=common_switch)


RMS_EPS = 1e-06
GROUP_EPS = 0.00064
HIGHEST = lax.Precision.HIGHEST

def rms_norm(values, norm_gain):
    mean_sq = lax.optimization_barrier(jnp.mean(values * values, axis=-1, keepdims=True))
    return values * lax.rsqrt(mean_sq + RMS_EPS) * norm_gain

def split_product(left_rows, weight_rows):
    block_width = left_rows.shape[1] // N_TP
    running = jnp.zeros((left_rows.shape[0], weight_rows.shape[1]), jnp.float32)
    for block_index in range(N_TP):
        lower = block_index * block_width
        product = jnp.dot(left_rows[:, lower:lower + block_width], weight_rows[lower:lower + block_width], preferred_element_type=jnp.float32)
        running = running + lax.optimization_barrier(product.astype(jnp.bfloat16)).astype(jnp.float32)
    return running.astype(jnp.bfloat16)

def evolve_memory(memory_arrays, receiver_lanes, address_lanes, content_lanes, forget_lanes, learning_lanes, lane_rescale, instant_reward):
    unit_key = address_lanes * lax.rsqrt(lax.optimization_barrier(jnp.sum(address_lanes * address_lanes, axis=-1, keepdims=True)) + 1.0)
    stepped_address = address_lanes * learning_lanes
    removal = jnp.einsum('bhvk,bhk->bhv', memory_arrays, unit_key, precision=HIGHEST)
    memory_after = memory_arrays * forget_lanes[:, :, None, :] - removal[..., None] * (unit_key * learning_lanes)[:, :, None, :] + content_lanes[..., None] * stepped_address[:, :, None, :]
    memory_retrieval = jnp.einsum('bhvk,bhk->bhv', memory_after, receiver_lanes, precision=HIGHEST)
    centred = memory_retrieval - lax.optimization_barrier(jnp.mean(memory_retrieval, axis=-1, keepdims=True))
    unit_address = centred * lax.rsqrt(lax.optimization_barrier(jnp.mean(centred * centred, axis=-1, keepdims=True)) + GROUP_EPS)
    instant_extra = lax.optimization_barrier(jnp.sum(receiver_lanes * stepped_address * instant_reward, axis=-1, keepdims=True)) * content_lanes
    return (memory_after, unit_address * lane_rescale + instant_extra)

def swiglu(rows_in, gate_w, up_w):
    gate_val = jnp.dot(rows_in, gate_w, preferred_element_type=jnp.float32)
    up_val = jnp.dot(rows_in, up_w, preferred_element_type=jnp.float32)
    return (jax.nn.silu(gate_val) * up_val).astype(jnp.bfloat16)

def reference(fresh_inputs, memory_arrays, chosen_specialist, chosen_coefficient, first_rescale, second_rescale, receiver_projector, address_projector, content_projector, final_projector, forget_narrowing, forget_widening, forget_bias, learning_narrowing, learning_widening, learning_bias, lane_scaling, instant_reward, specialist_switch, specialist_expand, specialist_contract, common_activator, common_expand, common_contract, common_switch):
    batch_rows = fresh_inputs.shape[0]
    residual = fresh_inputs.astype(jnp.float32)
    normed = rms_norm(residual, first_rescale).astype(jnp.bfloat16)
    receiver_array = split_product(normed, receiver_projector)
    address_mapped = split_product(normed, address_projector)
    content_array = split_product(normed, content_projector)
    decay_mid = jnp.tanh(jnp.dot(normed, forget_narrowing, preferred_element_type=jnp.float32)).astype(jnp.bfloat16)
    decay_pre = forget_bias + jnp.dot(decay_mid, forget_widening, preferred_element_type=jnp.float32)
    forget_multiplier = jnp.exp(-jnp.exp(-jax.nn.softplus(-decay_pre) - 0.5))
    rate_mid = jnp.dot(normed, learning_narrowing, preferred_element_type=jnp.float32).astype(jnp.bfloat16)
    learning_step = jax.nn.sigmoid(learning_bias + jnp.dot(rate_mid, learning_widening, preferred_element_type=jnp.float32))

    def divide_lanes(channels):
        return channels.astype(jnp.float32).reshape(batch_rows, LANE_COUNT, LANE_WIDTH)
    memory_after, memory_retrieval = evolve_memory(memory_arrays, divide_lanes(receiver_array), divide_lanes(address_mapped), divide_lanes(content_array), divide_lanes(forget_multiplier), divide_lanes(learning_step), lane_scaling.reshape(LANE_COUNT, LANE_WIDTH), instant_reward)
    attended = memory_retrieval.reshape(batch_rows, MODEL_DIM).astype(jnp.bfloat16)
    mixed = split_product(attended, final_projector)
    residual = residual + mixed.astype(jnp.float32)
    ffn_in = rms_norm(residual, second_rescale).astype(jnp.bfloat16)
    routed = jnp.zeros((batch_rows, MODEL_DIM), jnp.float32)
    for expert in range(EXPERTS):
        lower = expert * FF_E
        hidden = swiglu(ffn_in, specialist_switch[:, lower:lower + FF_E], specialist_expand[:, lower:lower + FF_E])
        share = lax.optimization_barrier(jnp.sum(jnp.where(chosen_specialist == expert, chosen_coefficient.astype(jnp.float32), 0.0), axis=1))
        routed = routed + share[:, None] * jnp.dot(hidden, specialist_contract[lower:lower + FF_E], preferred_element_type=jnp.float32)
    shared_hidden = swiglu(ffn_in, common_activator, common_expand)
    branch_scale = jax.nn.sigmoid(jnp.dot(ffn_in, common_switch, preferred_element_type=jnp.float32))
    routed = routed + branch_scale[:, None] * jnp.dot(shared_hidden, common_contract, preferred_element_type=jnp.float32)
    return ((residual + routed).astype(jnp.bfloat16), memory_after)
```

```python
import functools
import math

import jax
import jax.numpy as jnp
from jax import lax
from jax.experimental import pallas as pl
from jax.experimental.pallas import tpu as pltpu
from jax.sharding import PartitionSpec as P

LANE_WIDTH = 64
FF_E = 7168


RMS_EPS = 1e-06
GROUP_EPS = 0.00064
HIGHEST = lax.Precision.HIGHEST
MESH = pl.DeviceIdType.MESH
VMEM_ROOM = 40 * 2**20


def rms_norm(values, norm_gain):
    mean_sq = jnp.mean(values * values, axis=-1, keepdims=True)
    return values * lax.rsqrt(mean_sq + RMS_EPS) * norm_gain


def widen(rounded):
    return lax.optimization_barrier(rounded).astype(jnp.float32)


def evolve_memory(
    memory_arrays,
    receiver_lanes,
    address_lanes,
    content_lanes,
    forget_lanes,
    learning_lanes,
    lane_rescale,
    instant_reward,
):
    unit_key = address_lanes * lax.rsqrt(
        jnp.sum(address_lanes * address_lanes, axis=-1, keepdims=True) + 1.0
    )
    stepped_address = address_lanes * learning_lanes
    removal = jnp.einsum("bhvk,bhk->bhv", memory_arrays, unit_key, precision=HIGHEST)
    memory_after = (
        memory_arrays * forget_lanes[:, :, None, :]
        - removal[..., None] * (unit_key * learning_lanes)[:, :, None, :]
        + content_lanes[..., None] * stepped_address[:, :, None, :]
    )
    memory_retrieval = jnp.einsum("bhvk,bhk->bhv", memory_after, receiver_lanes, precision=HIGHEST)
    centred = memory_retrieval - jnp.mean(memory_retrieval, axis=-1, keepdims=True)
    unit_address = centred * lax.rsqrt(
        jnp.mean(centred * centred, axis=-1, keepdims=True) + GROUP_EPS
    )
    instant_extra = (
        jnp.sum(receiver_lanes * stepped_address * instant_reward, axis=-1, keepdims=True)
        * content_lanes
    )
    return (memory_after, unit_address * lane_rescale + instant_extra)


def swiglu(rows_in, gate_w, up_w):
    gate_val = jnp.dot(rows_in, gate_w, preferred_element_type=jnp.float32)
    up_val = jnp.dot(rows_in, up_w, preferred_element_type=jnp.float32)
    return (jax.nn.silu(gate_val) * up_val).astype(jnp.bfloat16)


def body(
    fresh_inputs,
    memory_arrays,
    chosen_specialist,
    chosen_coefficient,
    first_rescale,
    second_rescale,
    receiver_projector,
    address_projector,
    content_projector,
    final_projector,
    forget_narrowing,
    forget_widening,
    forget_bias,
    learning_narrowing,
    learning_widening,
    learning_bias,
    lane_scaling,
    instant_reward,
    specialist_switch,
    specialist_expand,
    specialist_contract,
    common_activator,
    common_expand,
    common_contract,
    common_switch,
):
    own_rows = fresh_inputs.shape[0]
    model_width = fresh_inputs.shape[1]
    tp_count = lax.axis_size("tp")
    tp_rank = lax.axis_index("tp")
    half_width = model_width // tp_count
    head_count = half_width // LANE_WIDTH
    residual = fresh_inputs.astype(jnp.float32)
    normed = rms_norm(residual, first_rescale).astype(jnp.bfloat16)
    normed_half = lax.dynamic_slice_in_dim(normed, tp_rank * half_width, half_width, 1)
    local_weights = jnp.stack((receiver_projector, address_projector, content_projector), axis=1)
    projected_rows = jnp.einsum(
        "rd,dkc->rkc",
        lax.all_gather(normed_half, "ep", axis=0, tiled=True),
        local_weights,
        preferred_element_type=jnp.float32,
    ).astype(jnp.bfloat16)
    partial_value = lax.all_to_all(projected_rows, "ep", split_axis=0, concat_axis=2, tiled=True)
    projected = lax.psum(widen(partial_value).astype(jnp.bfloat16), "tp")
    mine = lax.dynamic_slice_in_dim(projected, tp_rank * half_width, half_width, 2)

    def divide_lanes(channels):
        return channels.astype(jnp.float32).reshape(own_rows, head_count, LANE_WIDTH)

    decay_mid = jnp.tanh(
        jnp.dot(normed, forget_narrowing, preferred_element_type=jnp.float32)
    ).astype(jnp.bfloat16)
    decay_pre = forget_bias + jnp.dot(
        decay_mid, forget_widening, preferred_element_type=jnp.float32
    )
    decay_vals = jnp.exp(-jnp.exp(-jax.nn.softplus(-decay_pre) - 0.5))
    rate_mid = jnp.dot(normed, learning_narrowing, preferred_element_type=jnp.float32).astype(
        jnp.bfloat16
    )
    rate_vals = jax.nn.sigmoid(
        learning_bias + jnp.dot(rate_mid, learning_widening, preferred_element_type=jnp.float32)
    )
    memory_after, memory_retrieval = evolve_memory(
        memory_arrays,
        divide_lanes(mine[:, 0]),
        divide_lanes(mine[:, 1]),
        divide_lanes(mine[:, 2]),
        divide_lanes(decay_vals),
        divide_lanes(rate_vals),
        lane_scaling.reshape(head_count, LANE_WIDTH),
        instant_reward,
    )
    attended = memory_retrieval.reshape(own_rows, half_width).astype(jnp.bfloat16)
    done_rows = jnp.dot(
        lax.all_gather(attended, "ep", axis=0, tiled=True),
        final_projector,
        preferred_element_type=jnp.float32,
    ).astype(jnp.bfloat16)
    out_part = lax.all_to_all(done_rows, "ep", split_axis=0, concat_axis=1, tiled=True)
    mixed_out = lax.psum(widen(out_part).astype(jnp.bfloat16), "tp")
    residual = residual + mixed_out.astype(jnp.float32)
    ffn_in = rms_norm(residual, second_rescale).astype(jnp.bfloat16)
    all_in, all_weight, all_ids = (
        lax.all_gather(ffn_in, "ep", axis=0, tiled=True),
        lax.all_gather(chosen_coefficient, "ep", axis=0, tiled=True),
        lax.all_gather(chosen_specialist, "ep", axis=0, tiled=True),
    )
    column_count = specialist_switch.shape[1]
    flat_rank = lax.axis_index("ep") * tp_count + tp_rank
    expert = flat_rank * column_count // FF_E
    expert_share = jnp.sum(
        jnp.where(all_ids == expert, all_weight.astype(jnp.float32), 0.0), axis=1
    )
    hidden = swiglu(all_in, specialist_switch, specialist_expand)
    shared_hidden = swiglu(all_in, common_activator, common_expand)
    branch_scale = jax.nn.sigmoid(
        jnp.dot(all_in, common_switch, preferred_element_type=jnp.float32)
    )
    rows_mine = own_rows // tp_count
    expert_term = expert_share[:, None] * jnp.dot(
        hidden, specialist_contract, preferred_element_type=jnp.float32
    )
    routed = lax.psum_scatter(
        expert_term
        + branch_scale[:, None]
        * jnp.dot(shared_hidden, common_contract, preferred_element_type=jnp.float32),
        ("ep", "tp"),
        scatter_dimension=0,
        tiled=True,
    )
    own_residual = lax.dynamic_slice_in_dim(residual, tp_rank * rows_mine, rows_mine, 0)
    return ((own_residual + routed).astype(jnp.bfloat16), memory_after)


def _others(ep, tp, fn):
    me, core = lax.axis_index("ep"), lax.axis_index("tp")
    for far in range(ep):
        for side in range(tp):
            if far or side:
                fn(lax.rem(me + far, ep), lax.rem(core + side, tp))


def _meet(ep, tp):
    barrier = pltpu.get_barrier_semaphore()
    _others(
        ep,
        tp,
        lambda e, t: pl.semaphore_signal(
            barrier, inc=1, device_id={"ep": e, "tp": t}, device_id_type=MESH
        ),
    )
    pl.semaphore_wait(barrier, ep * tp - 1)


def _remote(src, dst, send, recv, e, t):
    return pltpu.make_async_remote_copy(
        src_ref=src,
        dst_ref=dst,
        send_sem=send,
        recv_sem=recv,
        device_id={"ep": e, "tp": t},
        device_id_type=MESH,
    )


def project_kernel(
    ep, tp, x, gain, wq, wk, wv, fnar, fwid, fbias, lnar, lwid, lbias,
    qkv, decay, rate,
    halves, rows_all, w, part, got, wsem, ssem, rsem, psem, gsem, lsem,
):
    me, core = lax.axis_index("ep"), lax.axis_index("tp")
    group = ep // tp
    loads = [pltpu.make_async_copy(ref, w.at[i], wsem.at[i]) for i, ref in enumerate((wq, wk, wv))]
    for load in loads:
        load.start()
    own, width = x.shape
    half = width // tp
    values = x[...].astype(jnp.float32)
    normed = (rms_norm(values, gain[...])).astype(jnp.bfloat16)
    for i in range(tp):
        halves[i] = normed[:, i * half : (i + 1) * half]
    _meet(ep, tp)
    sends = []
    for far in range(1, ep):
        e = lax.rem(me + far, ep)
        sends.append(
            _remote(halves.at[core], rows_all.at[me], ssem.at[far], rsem.at[me], e, core)
        )
        sends[-1].start()
    rows_all[me] = halves[core]
    decay_mid = jnp.tanh(
        jnp.dot(normed, fnar[...], preferred_element_type=jnp.float32)
    ).astype(jnp.bfloat16)
    decay_pre = fbias[...] + jnp.dot(decay_mid, fwid[...], preferred_element_type=jnp.float32)
    decay[...] = jnp.exp(-(math.exp(-0.5) / (1.0 + jnp.exp(-decay_pre))))
    rate_mid = jnp.dot(normed, lnar[...], preferred_element_type=jnp.float32).astype(jnp.bfloat16)
    rate_pre = lbias[...] + jnp.dot(rate_mid, lwid[...], preferred_element_type=jnp.float32)
    rate[...] = 1.0 / (1.0 + jnp.exp(-rate_pre))
    for load in loads:
        load.wait()
    for far in range(1, ep):
        e = lax.rem(me + far, ep)
        pltpu.make_async_copy(rows_all.at[e], rows_all.at[e], rsem.at[e]).wait()
    every = rows_all[...].reshape(ep * own, half)
    for i in range(3):
        done = jnp.dot(every, w[i], preferred_element_type=jnp.float32)
        part[:, i] = done.astype(jnp.bfloat16).reshape(ep, own, done.shape[1])
    goal = me // group
    slot = core * group + lax.rem(me, group)
    for far in range(1, ep):
        e = lax.rem(me + far, ep)
        _remote(part.at[e], got.at[slot], psem.at[far], gsem.at[slot], e, goal).start()
    here = goal == core
    local = pltpu.make_async_copy(part.at[me], got.at[slot], gsem.at[slot])
    across = _remote(part.at[me], got.at[slot], psem.at[0], gsem.at[slot], me, goal)

    @pl.when(here)
    def _():
        local.start()

    @pl.when(jnp.logical_not(here))
    def _():
        across.start()

    for i in range(ep):
        pltpu.make_async_copy(got.at[i], got.at[i], gsem.at[i]).wait()
    cols = w.shape[2]
    for j in range(group):
        for i in range(3):
            total = got[j, i].astype(jnp.float32)
            for s in range(1, tp):
                total = total + got[s * group + j, i].astype(jnp.float32)
            qkv[i, :, j * cols : (j + 1) * cols] = total.astype(jnp.bfloat16)
    for send in sends:
        send.wait_send()
    for far in range(1, ep):
        _remote(part.at[me], got.at[slot], psem.at[far], gsem.at[slot], me, goal).wait_send()

    @pl.when(jnp.logical_not(here))
    def _():
        across.wait_send()


def ffn_kernel(
    ep, tp, expert_cols, att, x, ids, coef, gain, cs, wo_h, wg_h, wu_h, wd_h, cg_h, cu_h, cd_h,
    out,
    att_all, xcol, share, wo, wg, wu, wd, cg, cu, cd, pbuf, psib, res, ffn, hid, chid,
    sibout, sibin, mine, got,
    wsem, s_att, r_att, s_x, r_x, s_sh, r_sh, s_p, r_p, s_res, r_res, f_res, b_res,
    s_sib, r_sib, s_out, r_out,
):
    me, core = lax.axis_index("ep"), lax.axis_index("tp")
    mate = lax.rem(core + 1, tp)
    group = ep // tp
    own, width = x.shape
    cols = wo.shape[1]
    loads = [
        pltpu.make_async_copy(a, b, wsem.at[i])
        for i, (a, b) in enumerate(
            ((wo_h, wo), (wg_h, wg), (wu_h, wu), (cg_h, cg), (cu_h, cu), (wd_h, wd), (cd_h, cd))
        )
    ]
    for load in loads:
        load.start()
    lane = lax.broadcasted_iota(jnp.int32, (own, 128), 1)
    routes = jnp.zeros((own, 128), jnp.float32)
    for k in range(ids.shape[1]):
        routes = routes + jnp.where(
            ids[:, k : k + 1] == lane, coef[:, k : k + 1].astype(jnp.float32), 0.0
        )
    share[me] = routes
    _meet(ep, tp)
    sends = []

    def push(*args):
        sends.append(_remote(*args))
        sends[-1].start()

    for far in range(1, ep):
        e = lax.rem(me + far, ep)
        push(att, att_all.at[me], s_att.at[far], r_att.at[me], e, core)
    for far in range(1, ep):
        e = lax.rem(me + far, ep)
        block = x.at[:, pl.ds(pl.multiple_of(e * cols, cols), cols)]
        push(block, xcol.at[me], s_x.at[far], r_x.at[me], e, core)
        push(share.at[me], share.at[me], s_sh.at[far], r_sh.at[me], e, core)
    att_all[me] = att[...]
    xcol[me] = x[:, pl.ds(pl.multiple_of(me * cols, cols), cols)]
    loads[0].wait()

    def arrive(ref, sem):
        pltpu.make_async_copy(ref, ref, sem).wait()

    for far in range(1, ep):
        e = lax.rem(me + far, ep)
        arrive(att_all.at[e], r_att.at[e])
    half = att.shape[1]
    done = jnp.dot(
        att_all[...].reshape(ep * own, half), wo[...], preferred_element_type=jnp.float32
    ).astype(jnp.bfloat16)
    pbuf[...] = done.reshape(tp, group * own, cols)
    push(pbuf.at[mate], psib, s_p, r_p, me, mate)
    for far in range(1, ep):
        e = lax.rem(me + far, ep)
        arrive(xcol.at[e], r_x.at[e])
    arrive(psib, r_p)
    mixed = (pbuf[core].astype(jnp.float32) + psib[...].astype(jnp.float32)).astype(jnp.bfloat16)
    held = xcol[pl.ds(core * group, group)].reshape(group * own, cols).astype(jnp.float32)
    res[me, core] = (held + mixed.astype(jnp.float32)).astype(jnp.bfloat16)
    for far in range(1, ep):
        e = lax.rem(me + far, ep)
        push(res.at[me, core], res.at[me, core], s_res.at[far], r_res.at[me], e, core)
    push(res.at[me, core], res.at[me, core], f_res.at[me], b_res.at[me], me, mate)
    for far in range(1, ep):
        e = lax.rem(me + far, ep)
        arrive(res.at[e, core], r_res.at[e])
        push(res.at[e, core], res.at[e, core], f_res.at[e], b_res.at[e], me, mate)
    for far in range(ep):
        e = lax.rem(me + far, ep)
        arrive(res.at[e, mate], b_res.at[e])
    rows = ep * own
    square = jnp.zeros((rows, 1), jnp.float32)
    for s in range(ep):
        block = res[s].reshape(rows, cols).astype(jnp.float32)
        square = square + jnp.sum(block * block, axis=-1, keepdims=True)
    inv = lax.rsqrt(square / width + RMS_EPS)
    gate_sum = jnp.zeros((rows, 1), jnp.float32)
    for s in range(ep):
        at = slice(s * cols, (s + 1) * cols)
        block = res[s].reshape(rows, cols).astype(jnp.float32)
        block = (block * inv * gain[:, at]).astype(jnp.bfloat16)
        ffn[:, at] = block
        gate_sum = gate_sum + jnp.sum(
            block.astype(jnp.float32) * cs[:, at].astype(jnp.float32), axis=-1, keepdims=True
        )
    branch_scale = 1.0 / (1.0 + jnp.exp(-gate_sum))
    for far in range(1, ep):
        e = lax.rem(me + far, ep)
        arrive(share.at[e], r_sh.at[e])
    expert = (me * tp + core) * wg.shape[1] // expert_cols
    table = share[...].reshape(rows, 128)
    picked = lax.broadcasted_iota(jnp.int32, (rows, 128), 1) == expert
    weight = jnp.sum(jnp.where(picked, table, 0.0), axis=-1, keepdims=True)
    for i in (1, 2):
        loads[i].wait()

    def widen_up(c, _):
        at = pl.ds(pl.multiple_of(c * 256, 256), 256)
        g = jnp.dot(ffn[...], wg[:, at], preferred_element_type=jnp.float32)
        u = jnp.dot(ffn[...], wu[:, at], preferred_element_type=jnp.float32)
        hid[:, at] = (g / (1.0 + jnp.exp(-g)) * u).astype(jnp.bfloat16)
        return _

    lax.fori_loop(0, wg.shape[1] // 256, widen_up, 0)
    for i in (3, 4):
        loads[i].wait()
    g = jnp.dot(ffn[...], cg[...], preferred_element_type=jnp.float32)
    u = jnp.dot(ffn[...], cu[...], preferred_element_type=jnp.float32)
    chid[...] = (g / (1.0 + jnp.exp(-g)) * u).astype(jnp.bfloat16)
    for i in (5, 6):
        loads[i].wait()
    pieces = mine.shape[0]
    piece = width // pieces
    last = own // tp
    for n in range(pieces):
        at = slice(n * piece, (n + 1) * piece)
        y = weight * jnp.dot(hid[...], wd[:, at], preferred_element_type=jnp.float32)
        y = y + branch_scale * jnp.dot(chid[...], cd[:, at], preferred_element_type=jnp.float32)
        y = y.reshape(ep, tp, last, piece)
        for side in range(tp):
            sibout[n, side] = y[:, side].astype(jnp.bfloat16)
        push(sibout.at[n, mate], sibin.at[n], s_sib.at[n], r_sib.at[n], me, mate)
    for n in range(pieces):
        arrive(sibin.at[n], r_sib.at[n])
        mine[n] = (
            sibout[n, core].astype(jnp.float32) + sibin[n].astype(jnp.float32)
        ).astype(jnp.bfloat16)
        for far in range(1, ep):
            e = lax.rem(me + far, ep)
            push(mine.at[n, e], got.at[n, me], s_out.at[n, far], r_out.at[n, me], e, core)
    start = pl.multiple_of(lax.rem(me, group) * own, own)
    per = piece // cols
    for n in range(pieces):
        total = mine[n, me].astype(jnp.float32)
        for far in range(1, ep):
            e = lax.rem(me + far, ep)
            arrive(got.at[n, e], r_out.at[n, e])
            total = total + got[n, e].astype(jnp.float32)
        for s in range(per):
            base = res[n * per + s, me // group, pl.ds(start, own)].astype(jnp.float32)
            base = jnp.where(core == 0, base[:last], base[last:])
            a = n * piece + s * cols
            out[:, a : a + cols] = (base + total[:, s * cols : (s + 1) * cols]).astype(jnp.bfloat16)
    for send in sends:
        send.wait_send()


def layer(*blocks):
    own = blocks[0].shape[0]
    cols, hidden = blocks[9].shape[1], blocks[18].shape[1]
    tiles = cols % 128 == 0 and hidden % 256 == 0 and own % 16 == 0
    heads_match = lax.axis_size("ep") % lax.axis_size("tp") == 0 and lax.axis_size("tp") == 2
    weights = sum(2 * w.size for w in blocks[18:24])
    rows = own * lax.axis_size("ep")
    held = weights + rows * (12 * blocks[0].shape[1] + 8 * hidden)
    small = held < VMEM_ROOM
    return (kernel_body if tiles and heads_match and small else body)(*blocks)


def kernel_body(
    fresh_inputs,
    memory_arrays,
    chosen_specialist,
    chosen_coefficient,
    first_rescale,
    second_rescale,
    receiver_projector,
    address_projector,
    content_projector,
    final_projector,
    forget_narrowing,
    forget_widening,
    forget_bias,
    learning_narrowing,
    learning_widening,
    learning_bias,
    lane_scaling,
    instant_reward,
    specialist_switch,
    specialist_expand,
    specialist_contract,
    common_activator,
    common_expand,
    common_contract,
    common_switch,
):
    ep, tp = lax.axis_size("ep"), lax.axis_size("tp")
    own, width = fresh_inputs.shape
    half, cols = width // tp, final_projector.shape[1]
    heads = half // LANE_WIDTH
    group = ep // tp
    vmem = pl.BlockSpec(memory_space=pltpu.VMEM)
    hbm = pl.BlockSpec(memory_space=pl.ANY)
    bf16, f32 = jnp.bfloat16, jnp.float32
    dma = pltpu.SemaphoreType.DMA

    def row(vector):
        return vector.reshape(1, -1)

    qkv, decay_vals, rate_vals = pl.pallas_call(
        functools.partial(project_kernel, ep, tp),
        out_shape=(
            jax.ShapeDtypeStruct((3, own, half), bf16),
            jax.ShapeDtypeStruct((own, half), f32),
            jax.ShapeDtypeStruct((own, half), f32),
        ),
        in_specs=[vmem] * 2 + [hbm] * 3 + [vmem] * 6,
        out_specs=(vmem,) * 3,
        scratch_shapes=[
            pltpu.VMEM((tp, own, half), bf16),
            pltpu.VMEM((ep, own, half), bf16),
            pltpu.VMEM((3, half, cols), bf16),
            pltpu.VMEM((ep, 3, own, cols), bf16),
            pltpu.VMEM((ep, 3, own, cols), bf16),
            dma((3,)),
            dma((ep,)),
            dma((ep,)),
            dma((ep,)),
            dma((ep,)),
            dma((1,)),
        ],
        compiler_params=pltpu.CompilerParams(collective_id=0, has_side_effects=True),
        name="project",
    )(
        fresh_inputs,
        row(first_rescale),
        receiver_projector,
        address_projector,
        content_projector,
        forget_narrowing,
        forget_widening,
        row(forget_bias),
        learning_narrowing,
        learning_widening,
        row(learning_bias),
    )

    def divide_lanes(channels):
        return channels.astype(jnp.float32).reshape(own, heads, LANE_WIDTH)

    memory_after, memory_retrieval = evolve_memory(
        memory_arrays,
        divide_lanes(qkv[0]),
        divide_lanes(qkv[1]),
        divide_lanes(qkv[2]),
        divide_lanes(decay_vals),
        divide_lanes(rate_vals),
        lane_scaling.reshape(heads, LANE_WIDTH),
        instant_reward,
    )
    attended = memory_retrieval.reshape(own, half).astype(jnp.bfloat16)
    rows, hidden, dense = ep * own, specialist_switch.shape[1], common_activator.shape[1]
    pieces = 4
    piece, last = width // pieces, own // tp
    new_tokens = pl.pallas_call(
        functools.partial(ffn_kernel, ep, tp, FF_E),
        out_shape=jax.ShapeDtypeStruct((last, width), bf16),
        in_specs=[vmem] * 6 + [hbm] * 7,
        out_specs=vmem,
        scratch_shapes=[
            pltpu.VMEM((ep, own, half), bf16),
            pltpu.VMEM((ep, own, cols), bf16),
            pltpu.VMEM((ep, own, 128), f32),
            pltpu.VMEM((half, cols), bf16),
            pltpu.VMEM((width, hidden), bf16),
            pltpu.VMEM((width, hidden), bf16),
            pltpu.VMEM((hidden, width), bf16),
            pltpu.VMEM((width, dense), bf16),
            pltpu.VMEM((width, dense), bf16),
            pltpu.VMEM((dense, width), bf16),
            pltpu.VMEM((tp, group * own, cols), bf16),
            pltpu.VMEM((group * own, cols), bf16),
            pltpu.VMEM((ep, tp, group * own, cols), bf16),
            pltpu.VMEM((rows, width), bf16),
            pltpu.VMEM((rows, hidden), bf16),
            pltpu.VMEM((rows, dense), bf16),
            pltpu.VMEM((pieces, tp, ep, last, piece), bf16),
            pltpu.VMEM((pieces, ep, last, piece), bf16),
            pltpu.VMEM((pieces, ep, last, piece), bf16),
            pltpu.VMEM((pieces, ep, last, piece), bf16),
            dma((7,)),
            dma((ep,)),
            dma((ep,)),
            dma((ep,)),
            dma((ep,)),
            dma((ep,)),
            dma((ep,)),
            dma,
            dma,
            dma((ep,)),
            dma((ep,)),
            dma((ep,)),
            dma((ep,)),
            dma((pieces,)),
            dma((pieces,)),
            dma((pieces, ep)),
            dma((pieces, ep)),
        ],
        compiler_params=pltpu.CompilerParams(
            collective_id=1, has_side_effects=True, vmem_limit_bytes=56 * 2**20
        ),
        name="experts",
    )(
        attended,
        fresh_inputs,
        chosen_specialist,
        chosen_coefficient,
        row(second_rescale),
        row(common_switch),
        final_projector,
        specialist_switch,
        specialist_expand,
        specialist_contract,
        common_activator,
        common_expand,
        common_contract,
    )
    return (new_tokens, memory_after)


def solution(mesh):
    placed = (
        P(("grp", "ep"), None),
        P(("grp", "ep"), "tp", None, None),
        P(("grp", "ep"), None),
        P(("grp", "ep"), None),
        P(),
        P(),
        P("tp", "ep"),
        P("tp", "ep"),
        P("tp", "ep"),
        P("tp", "ep"),
        P(),
        P(None, "tp"),
        P("tp"),
        P(),
        P(None, "tp"),
        P("tp"),
        P("tp"),
        P("tp", None),
        P(None, ("ep", "tp")),
        P(None, ("ep", "tp")),
        P(("ep", "tp"), None),
        P(None, ("ep", "tp")),
        P(None, ("ep", "tp")),
        P(("ep", "tp"), None),
        P(),
    )
    return jax.shard_map(
        layer,
        mesh=mesh,
        in_specs=placed,
        out_specs=(P(("grp", "ep", "tp"), None), P(("grp", "ep"), "tp", None, None)),
        check_vma=False,
    )
```

```python
import functools
import math

import jax
import jax.numpy as jnp
from jax import lax
from jax.experimental import pallas as pl
from jax.experimental.pallas import tpu as pltpu
from jax.sharding import PartitionSpec as P

LANE_WIDTH = 64
FF_E = 7168


RMS_EPS = 1e-06
GROUP_EPS = 0.00064
HIGHEST = lax.Precision.HIGHEST
MESH = pl.DeviceIdType.MESH
VMEM_ROOM = 40 * 2**20


def rms_norm(values, norm_gain):
    mean_sq = jnp.mean(values * values, axis=-1, keepdims=True)
    return values * lax.rsqrt(mean_sq + RMS_EPS) * norm_gain


def widen(rounded):
    return lax.optimization_barrier(rounded).astype(jnp.float32)


def evolve_memory(
    memory_arrays,
    receiver_lanes,
    address_lanes,
    content_lanes,
    forget_lanes,
    learning_lanes,
    lane_rescale,
    instant_reward,
):
    unit_key = address_lanes * lax.rsqrt(
        jnp.sum(address_lanes * address_lanes, axis=-1, keepdims=True) + 1.0
    )
    stepped_address = address_lanes * learning_lanes
    removal = jnp.einsum("bhvk,bhk->bhv", memory_arrays, unit_key, precision=HIGHEST)
    memory_after = (
        memory_arrays * forget_lanes[:, :, None, :]
        - removal[..., None] * (unit_key * learning_lanes)[:, :, None, :]
        + content_lanes[..., None] * stepped_address[:, :, None, :]
    )
    memory_retrieval = jnp.einsum("bhvk,bhk->bhv", memory_after, receiver_lanes, precision=HIGHEST)
    centred = memory_retrieval - jnp.mean(memory_retrieval, axis=-1, keepdims=True)
    unit_address = centred * lax.rsqrt(
        jnp.mean(centred * centred, axis=-1, keepdims=True) + GROUP_EPS
    )
    instant_extra = (
        jnp.sum(receiver_lanes * stepped_address * instant_reward, axis=-1, keepdims=True)
        * content_lanes
    )
    return (memory_after, unit_address * lane_rescale + instant_extra)


def swiglu(rows_in, gate_w, up_w):
    gate_val = jnp.dot(rows_in, gate_w, preferred_element_type=jnp.float32)
    up_val = jnp.dot(rows_in, up_w, preferred_element_type=jnp.float32)
    return (jax.nn.silu(gate_val) * up_val).astype(jnp.bfloat16)


def body(
    fresh_inputs,
    memory_arrays,
    chosen_specialist,
    chosen_coefficient,
    first_rescale,
    second_rescale,
    receiver_projector,
    address_projector,
    content_projector,
    final_projector,
    forget_narrowing,
    forget_widening,
    forget_bias,
    learning_narrowing,
    learning_widening,
    learning_bias,
    lane_scaling,
    instant_reward,
    specialist_switch,
    specialist_expand,
    specialist_contract,
    common_activator,
    common_expand,
    common_contract,
    common_switch,
):
    own_rows = fresh_inputs.shape[0]
    model_width = fresh_inputs.shape[1]
    tp_count = lax.axis_size("tp")
    tp_rank = lax.axis_index("tp")
    half_width = model_width // tp_count
    head_count = half_width // LANE_WIDTH
    residual = fresh_inputs.astype(jnp.float32)
    normed = rms_norm(residual, first_rescale).astype(jnp.bfloat16)
    normed_half = lax.dynamic_slice_in_dim(normed, tp_rank * half_width, half_width, 1)
    local_weights = jnp.stack((receiver_projector, address_projector, content_projector), axis=1)
    projected_rows = jnp.einsum(
        "rd,dkc->rkc",
        lax.all_gather(normed_half, "ep", axis=0, tiled=True),
        local_weights,
        preferred_element_type=jnp.float32,
    ).astype(jnp.bfloat16)
    partial_value = lax.all_to_all(projected_rows, "ep", split_axis=0, concat_axis=2, tiled=True)
    projected = lax.psum(widen(partial_value).astype(jnp.bfloat16), "tp")
    mine = lax.dynamic_slice_in_dim(projected, tp_rank * half_width, half_width, 2)

    def divide_lanes(channels):
        return channels.astype(jnp.float32).reshape(own_rows, head_count, LANE_WIDTH)

    decay_mid = jnp.tanh(
        jnp.dot(normed, forget_narrowing, preferred_element_type=jnp.float32)
    ).astype(jnp.bfloat16)
    decay_pre = forget_bias + jnp.dot(
        decay_mid, forget_widening, preferred_element_type=jnp.float32
    )
    decay_vals = jnp.exp(-jnp.exp(-jax.nn.softplus(-decay_pre) - 0.5))
    rate_mid = jnp.dot(normed, learning_narrowing, preferred_element_type=jnp.float32).astype(
        jnp.bfloat16
    )
    rate_vals = jax.nn.sigmoid(
        learning_bias + jnp.dot(rate_mid, learning_widening, preferred_element_type=jnp.float32)
    )
    memory_after, memory_retrieval = evolve_memory(
        memory_arrays,
        divide_lanes(mine[:, 0]),
        divide_lanes(mine[:, 1]),
        divide_lanes(mine[:, 2]),
        divide_lanes(decay_vals),
        divide_lanes(rate_vals),
        lane_scaling.reshape(head_count, LANE_WIDTH),
        instant_reward,
    )
    attended = memory_retrieval.reshape(own_rows, half_width).astype(jnp.bfloat16)
    done_rows = jnp.dot(
        lax.all_gather(attended, "ep", axis=0, tiled=True),
        final_projector,
        preferred_element_type=jnp.float32,
    ).astype(jnp.bfloat16)
    out_part = lax.all_to_all(done_rows, "ep", split_axis=0, concat_axis=1, tiled=True)
    mixed_out = lax.psum(widen(out_part).astype(jnp.bfloat16), "tp")
    residual = residual + mixed_out.astype(jnp.float32)
    ffn_in = rms_norm(residual, second_rescale).astype(jnp.bfloat16)
    all_in, all_weight, all_ids = (
        lax.all_gather(ffn_in, "ep", axis=0, tiled=True),
        lax.all_gather(chosen_coefficient, "ep", axis=0, tiled=True),
        lax.all_gather(chosen_specialist, "ep", axis=0, tiled=True),
    )
    column_count = specialist_switch.shape[1]
    flat_rank = lax.axis_index("ep") * tp_count + tp_rank
    expert = flat_rank * column_count // FF_E
    expert_share = jnp.sum(
        jnp.where(all_ids == expert, all_weight.astype(jnp.float32), 0.0), axis=1
    )
    hidden = swiglu(all_in, specialist_switch, specialist_expand)
    shared_hidden = swiglu(all_in, common_activator, common_expand)
    branch_scale = jax.nn.sigmoid(
        jnp.dot(all_in, common_switch, preferred_element_type=jnp.float32)
    )
    rows_mine = own_rows // tp_count
    expert_term = expert_share[:, None] * jnp.dot(
        hidden, specialist_contract, preferred_element_type=jnp.float32
    )
    routed = lax.psum_scatter(
        expert_term
        + branch_scale[:, None]
        * jnp.dot(shared_hidden, common_contract, preferred_element_type=jnp.float32),
        ("ep", "tp"),
        scatter_dimension=0,
        tiled=True,
    )
    own_residual = lax.dynamic_slice_in_dim(residual, tp_rank * rows_mine, rows_mine, 0)
    return ((own_residual + routed).astype(jnp.bfloat16), memory_after)


def _others(ep, tp, fn):
    me, core = lax.axis_index("ep"), lax.axis_index("tp")
    for far in range(ep):
        for side in range(tp):
            if far or side:
                fn(lax.rem(me + far, ep), lax.rem(core + side, tp))


def _meet(ep, tp):
    barrier = pltpu.get_barrier_semaphore()
    _others(
        ep,
        tp,
        lambda e, t: pl.semaphore_signal(
            barrier, inc=1, device_id={"ep": e, "tp": t}, device_id_type=MESH
        ),
    )
    pl.semaphore_wait(barrier, ep * tp - 1)


def _remote(src, dst, send, recv, e, t):
    return pltpu.make_async_remote_copy(
        src_ref=src,
        dst_ref=dst,
        send_sem=send,
        recv_sem=recv,
        device_id={"ep": e, "tp": t},
        device_id_type=MESH,
    )


def across_dot(left, right):
    return lax.dot_general(
        left, right, (((1,), (1,)), ((), ())), preferred_element_type=jnp.float32
    )


def by_head(ref, channels, first):
    for h in range(channels.shape[1] // LANE_WIDTH):
        ref[:, first + h, :] = channels[:, h * LANE_WIDTH : (h + 1) * LANE_WIDTH]


def state_kernel(memory, query, key, value, decay, rate, lane_gain, reward, after, read, flip):
    count, heads = query.shape[0], query.shape[1]
    lane = lax.broadcasted_iota(jnp.int32, (LANE_WIDTH, 128), 1)

    def sequence(b, carry):
        q, k, v, d, r = query[b], key[b], value[b], decay[b], rate[b]
        unit = k * lax.rsqrt(jnp.sum(k * k, axis=-1, keepdims=True) + 1.0)
        scaled, pulled, seen = k * r, unit * r, d * q
        flip[0:heads] = v
        value_cols = flip[...].T
        found = jnp.zeros((LANE_WIDTH, 128), jnp.float32)
        for h in range(heads):
            one = slice(h, h + 1)
            m = memory[b, h]
            removal = jnp.sum(m * unit[one], axis=-1, keepdims=True)
            kept = jnp.sum(m * seen[one], axis=-1, keepdims=True)
            after[b, h] = m * d[one] - removal * pulled[one] + value_cols[:, one] * scaled[one]
            found = jnp.where(lane == h, removal, found)
            found = jnp.where(lane == heads + h, kept, found)
        rows = found.T
        out = (
            rows[heads : 2 * heads]
            - rows[0:heads] * jnp.sum(pulled * q, axis=-1, keepdims=True)
            + v * jnp.sum(scaled * q, axis=-1, keepdims=True)
        )
        centred = out - jnp.mean(out, axis=-1, keepdims=True)
        level = lax.rsqrt(jnp.mean(centred * centred, axis=-1, keepdims=True) + GROUP_EPS)
        extra = jnp.sum(q * scaled * reward[...], axis=-1, keepdims=True) * v
        read[b] = centred * level * lane_gain[...] + extra
        return carry

    flip[...] = jnp.zeros_like(flip)
    lax.fori_loop(0, count, sequence, 0)


def project_kernel(
    ep, tp, x, gain, wq, wk, wv, fnar, fwid, fbias, lnar, lwid, lbias, scaling,
    query, key, value, decay, rate, lane_gain,
    halves, rows_all, w, part, got, wsem, ssem, rsem, psem, gsem, lsem,
):
    me, core = lax.axis_index("ep"), lax.axis_index("tp")
    group = ep // tp
    loads = [pltpu.make_async_copy(ref, w.at[i], wsem.at[i]) for i, ref in enumerate((wq, wk, wv))]
    for load in loads:
        load.start()
    own, width = x.shape
    half = width // tp
    values = x[...].astype(jnp.float32)
    normed = (rms_norm(values, gain[...])).astype(jnp.bfloat16)
    for i in range(tp):
        halves[i] = normed[:, i * half : (i + 1) * half]
    _meet(ep, tp)
    sends = []
    for far in range(1, ep):
        e = lax.rem(me + far, ep)
        sends.append(
            _remote(halves.at[core], rows_all.at[me], ssem.at[far], rsem.at[me], e, core)
        )
        sends[-1].start()
    rows_all[me] = halves[core]
    decay_mid = jnp.tanh(across_dot(normed, fnar[...])).astype(jnp.bfloat16)
    decay_pre = fbias[...] + jnp.dot(decay_mid, fwid[...], preferred_element_type=jnp.float32)
    by_head(decay, jnp.exp(-(math.exp(-0.5) / (1.0 + jnp.exp(-decay_pre)))), 0)
    rate_mid = across_dot(normed, lnar[...]).astype(jnp.bfloat16)
    rate_pre = lbias[...] + jnp.dot(rate_mid, lwid[...], preferred_element_type=jnp.float32)
    by_head(rate, 1.0 / (1.0 + jnp.exp(-rate_pre)), 0)
    for h in range(lane_gain.shape[0]):
        lane_gain[h : h + 1] = scaling[:, h * LANE_WIDTH : (h + 1) * LANE_WIDTH]
    for load in loads:
        load.wait()
    for far in range(1, ep):
        e = lax.rem(me + far, ep)
        pltpu.make_async_copy(rows_all.at[e], rows_all.at[e], rsem.at[e]).wait()
    every = rows_all[...].reshape(ep * own, half)
    for i in range(3):
        done = jnp.dot(every, w[i], preferred_element_type=jnp.float32)
        part[:, i] = done.astype(jnp.bfloat16).reshape(ep, own, done.shape[1])
    goal = me // group
    slot = core * group + lax.rem(me, group)
    for far in range(1, ep):
        e = lax.rem(me + far, ep)
        _remote(part.at[e], got.at[slot], psem.at[far], gsem.at[slot], e, goal).start()
    here = goal == core
    local = pltpu.make_async_copy(part.at[me], got.at[slot], gsem.at[slot])
    across = _remote(part.at[me], got.at[slot], psem.at[0], gsem.at[slot], me, goal)

    @pl.when(here)
    def _():
        local.start()

    @pl.when(jnp.logical_not(here))
    def _():
        across.start()

    for i in range(ep):
        pltpu.make_async_copy(got.at[i], got.at[i], gsem.at[i]).wait()
    cols = w.shape[2]
    for j in range(group):
        for i in range(3):
            total = got[j, i].astype(jnp.float32)
            for s in range(1, tp):
                total = total + got[s * group + j, i].astype(jnp.float32)
            total = total.astype(jnp.bfloat16).astype(jnp.float32)
            by_head((query, key, value)[i], total, j * (cols // LANE_WIDTH))
    for send in sends:
        send.wait_send()
    for far in range(1, ep):
        _remote(part.at[me], got.at[slot], psem.at[far], gsem.at[slot], me, goal).wait_send()

    @pl.when(jnp.logical_not(here))
    def _():
        across.wait_send()


def ffn_kernel(
    ep, tp, expert_cols, read, x, ids, coef, gain, cs, wo_h, wg_h, wu_h, wd_h, cg_h, cu_h, cd_h,
    out,
    att, att_all, xcol, share, wo, wg, wu, wd, cg, cu, cd, pbuf, psib, res, ffn, hid, chid,
    sibout, sibin, mine, got,
    wsem, s_att, r_att, s_x, r_x, s_sh, r_sh, s_p, r_p, s_res, r_res, f_res, b_res,
    s_sib, r_sib, s_out, r_out,
):
    me, core = lax.axis_index("ep"), lax.axis_index("tp")
    mate = lax.rem(core + 1, tp)
    group = ep // tp
    own, width = x.shape
    cols = wo.shape[1]
    loads = [
        pltpu.make_async_copy(a, b, wsem.at[i])
        for i, (a, b) in enumerate(
            ((wo_h, wo), (wg_h, wg), (wu_h, wu), (cg_h, cg), (cu_h, cu), (wd_h, wd), (cd_h, cd))
        )
    ]
    for load in loads:
        load.start()
    lane = lax.broadcasted_iota(jnp.int32, (own, 128), 1)
    routes = jnp.zeros((own, 128), jnp.float32)
    ids_cols, coef_cols = ids[...].T, coef[...].astype(jnp.float32).T
    for k in range(ids.shape[0]):
        routes = routes + jnp.where(
            ids_cols[:, k : k + 1] == lane, coef_cols[:, k : k + 1], 0.0
        )
    share[me] = routes
    pack = 128 // LANE_WIDTH
    for h in range(0, read.shape[1], pack):
        joined = jnp.concatenate([read[:, h + i, :] for i in range(pack)], axis=-1)
        att[:, h * LANE_WIDTH : h * LANE_WIDTH + 128] = joined.astype(jnp.bfloat16)
    _meet(ep, tp)
    sends = []

    def push(*args):
        sends.append(_remote(*args))
        sends[-1].start()

    for far in range(1, ep):
        e = lax.rem(me + far, ep)
        push(att, att_all.at[me], s_att.at[far], r_att.at[me], e, core)
    for far in range(1, ep):
        e = lax.rem(me + far, ep)
        block = x.at[:, pl.ds(pl.multiple_of(e * cols, cols), cols)]
        push(block, xcol.at[me], s_x.at[far], r_x.at[me], e, core)
        push(share.at[me], share.at[me], s_sh.at[far], r_sh.at[me], e, core)
    att_all[me] = att[...]
    xcol[me] = x[:, pl.ds(pl.multiple_of(me * cols, cols), cols)]
    loads[0].wait()

    def arrive(ref, sem):
        pltpu.make_async_copy(ref, ref, sem).wait()

    for far in range(1, ep):
        e = lax.rem(me + far, ep)
        arrive(att_all.at[e], r_att.at[e])
    half = att.shape[1]
    done = jnp.dot(
        att_all[...].reshape(ep * own, half), wo[...], preferred_element_type=jnp.float32
    ).astype(jnp.bfloat16)
    pbuf[...] = done.reshape(tp, group * own, cols)
    push(pbuf.at[mate], psib, s_p, r_p, me, mate)
    for far in range(1, ep):
        e = lax.rem(me + far, ep)
        arrive(xcol.at[e], r_x.at[e])
    arrive(psib, r_p)
    mixed = (pbuf[core].astype(jnp.float32) + psib[...].astype(jnp.float32)).astype(jnp.bfloat16)
    held = xcol[pl.ds(core * group, group)].reshape(group * own, cols).astype(jnp.float32)
    res[me, core] = (held + mixed.astype(jnp.float32)).astype(jnp.bfloat16)
    for far in range(1, ep):
        e = lax.rem(me + far, ep)
        push(res.at[me, core], res.at[me, core], s_res.at[far], r_res.at[me], e, core)
    push(res.at[me, core], res.at[me, core], f_res.at[me], b_res.at[me], me, mate)
    for far in range(1, ep):
        e = lax.rem(me + far, ep)
        arrive(res.at[e, core], r_res.at[e])
        push(res.at[e, core], res.at[e, core], f_res.at[e], b_res.at[e], me, mate)
    for far in range(ep):
        e = lax.rem(me + far, ep)
        arrive(res.at[e, mate], b_res.at[e])
    rows = ep * own
    square = jnp.zeros((rows, 1), jnp.float32)
    for s in range(ep):
        block = res[s].reshape(rows, cols).astype(jnp.float32)
        square = square + jnp.sum(block * block, axis=-1, keepdims=True)
    inv = lax.rsqrt(square / width + RMS_EPS)
    gate_sum = jnp.zeros((rows, 1), jnp.float32)
    for s in range(ep):
        at = slice(s * cols, (s + 1) * cols)
        block = res[s].reshape(rows, cols).astype(jnp.float32)
        block = (block * inv * gain[:, at]).astype(jnp.bfloat16)
        ffn[:, at] = block
        gate_sum = gate_sum + jnp.sum(
            block.astype(jnp.float32) * cs[:, at].astype(jnp.float32), axis=-1, keepdims=True
        )
    branch_scale = 1.0 / (1.0 + jnp.exp(-gate_sum))
    for far in range(1, ep):
        e = lax.rem(me + far, ep)
        arrive(share.at[e], r_sh.at[e])
    expert = (me * tp + core) * wg.shape[1] // expert_cols
    table = share[...].reshape(rows, 128)
    picked = lax.broadcasted_iota(jnp.int32, (rows, 128), 1) == expert
    weight = jnp.sum(jnp.where(picked, table, 0.0), axis=-1, keepdims=True)
    for i in (1, 2):
        loads[i].wait()

    def widen_up(c, _):
        at = pl.ds(pl.multiple_of(c * 256, 256), 256)
        g = jnp.dot(ffn[...], wg[:, at], preferred_element_type=jnp.float32)
        u = jnp.dot(ffn[...], wu[:, at], preferred_element_type=jnp.float32)
        hid[:, at] = (g / (1.0 + jnp.exp(-g)) * u).astype(jnp.bfloat16)
        return _

    lax.fori_loop(0, wg.shape[1] // 256, widen_up, 0)
    for i in (3, 4):
        loads[i].wait()
    g, u = across_dot(ffn[...], cg[...]), across_dot(ffn[...], cu[...])
    chid[...] = (g / (1.0 + jnp.exp(-g)) * u).astype(jnp.bfloat16)
    for i in (5, 6):
        loads[i].wait()
    pieces = mine.shape[0]
    piece = width // pieces
    last = own // tp
    for n in range(pieces):
        at = slice(n * piece, (n + 1) * piece)
        y = weight * jnp.dot(hid[...], wd[:, at], preferred_element_type=jnp.float32)
        y = y + branch_scale * jnp.dot(chid[...], cd[:, at], preferred_element_type=jnp.float32)
        y = y.reshape(ep, tp, last, piece)
        for side in range(tp):
            sibout[n, side] = y[:, side].astype(jnp.bfloat16)
        push(sibout.at[n, mate], sibin.at[n], s_sib.at[n], r_sib.at[n], me, mate)
    for n in range(pieces):
        arrive(sibin.at[n], r_sib.at[n])
        mine[n] = (
            sibout[n, core].astype(jnp.float32) + sibin[n].astype(jnp.float32)
        ).astype(jnp.bfloat16)
        for far in range(1, ep):
            e = lax.rem(me + far, ep)
            push(mine.at[n, e], got.at[n, me], s_out.at[n, far], r_out.at[n, me], e, core)
    start = pl.multiple_of(lax.rem(me, group) * own, own)
    per = piece // cols
    for n in range(pieces):
        total = mine[n, me].astype(jnp.float32)
        for far in range(1, ep):
            e = lax.rem(me + far, ep)
            arrive(got.at[n, e], r_out.at[n, e])
            total = total + got[n, e].astype(jnp.float32)
        for s in range(per):
            base = res[n * per + s, me // group, pl.ds(start, own)].astype(jnp.float32)
            base = jnp.where(core == 0, base[:last], base[last:])
            a = n * piece + s * cols
            out[:, a : a + cols] = (base + total[:, s * cols : (s + 1) * cols]).astype(jnp.bfloat16)
    for send in sends:
        send.wait_send()


def layer(*blocks):
    own = blocks[0].shape[0]
    cols, hidden = blocks[9].shape[1], blocks[18].shape[1]
    tiles = cols % 128 == 0 and hidden % 256 == 0 and own % 16 == 0
    heads_match = lax.axis_size("ep") % lax.axis_size("tp") == 0 and lax.axis_size("tp") == 2
    weights = sum(2 * w.size for w in blocks[18:24])
    rows = own * lax.axis_size("ep")
    held = weights + rows * (12 * blocks[0].shape[1] + 8 * hidden)
    small = held < VMEM_ROOM
    return (kernel_body if tiles and heads_match and small else body)(*blocks)


def kernel_body(
    fresh_inputs,
    memory_arrays,
    chosen_specialist,
    chosen_coefficient,
    first_rescale,
    second_rescale,
    receiver_projector,
    address_projector,
    content_projector,
    final_projector,
    forget_narrowing,
    forget_widening,
    forget_bias,
    learning_narrowing,
    learning_widening,
    learning_bias,
    lane_scaling,
    instant_reward,
    specialist_switch,
    specialist_expand,
    specialist_contract,
    common_activator,
    common_expand,
    common_contract,
    common_switch,
):
    ep, tp = lax.axis_size("ep"), lax.axis_size("tp")
    own, width = fresh_inputs.shape
    half, cols = width // tp, final_projector.shape[1]
    heads = half // LANE_WIDTH
    group = ep // tp
    vmem = pl.BlockSpec(memory_space=pltpu.VMEM)
    hbm = pl.BlockSpec(memory_space=pl.ANY)
    bf16, f32 = jnp.bfloat16, jnp.float32
    dma = pltpu.SemaphoreType.DMA

    def row(vector):
        return vector.reshape(1, -1)

    per_head = jax.ShapeDtypeStruct((own, heads, LANE_WIDTH), f32)
    *lanes, lane_gain = pl.pallas_call(
        functools.partial(project_kernel, ep, tp),
        out_shape=(per_head,) * 5 + (jax.ShapeDtypeStruct((heads, LANE_WIDTH), f32),),
        in_specs=[vmem] * 2 + [hbm] * 3 + [vmem] * 7,
        out_specs=(vmem,) * 6,
        scratch_shapes=[
            pltpu.VMEM((tp, own, half), bf16),
            pltpu.VMEM((ep, own, half), bf16),
            pltpu.VMEM((3, half, cols), bf16),
            pltpu.VMEM((ep, 3, own, cols), bf16),
            pltpu.VMEM((ep, 3, own, cols), bf16),
            dma((3,)),
            dma((ep,)),
            dma((ep,)),
            dma((ep,)),
            dma((ep,)),
            dma((1,)),
        ],
        compiler_params=pltpu.CompilerParams(collective_id=0, has_side_effects=True),
        name="project",
    )(
        fresh_inputs,
        row(first_rescale),
        receiver_projector,
        address_projector,
        content_projector,
        forget_narrowing.T,
        forget_widening,
        row(forget_bias),
        learning_narrowing.T,
        learning_widening,
        row(learning_bias),
        row(lane_scaling),
    )
    step = 2
    lane_spec = pl.BlockSpec((step, heads, LANE_WIDTH), lambda i: (i, 0, 0))
    gain_spec = pl.BlockSpec((heads, LANE_WIDTH), lambda i: (0, 0))
    memory_spec = pl.BlockSpec((step, heads, LANE_WIDTH, LANE_WIDTH), lambda i: (i, 0, 0, 0))
    memory_after, read = pl.pallas_call(
        state_kernel,
        grid=(own // step,),
        out_shape=(jax.ShapeDtypeStruct(memory_arrays.shape, f32), per_head),
        in_specs=[memory_spec] + [lane_spec] * 5 + [gain_spec] * 2,
        out_specs=(memory_spec, lane_spec),
        scratch_shapes=[pltpu.VMEM((128, LANE_WIDTH), f32)],
        name="state",
    )(memory_arrays, *lanes, lane_gain, instant_reward)
    rows, hidden, dense = ep * own, specialist_switch.shape[1], common_activator.shape[1]
    pieces = 4
    piece, last = width // pieces, own // tp
    new_tokens = pl.pallas_call(
        functools.partial(ffn_kernel, ep, tp, FF_E),
        out_shape=jax.ShapeDtypeStruct((last, width), bf16),
        in_specs=[vmem] * 6 + [hbm] * 7,
        out_specs=vmem,
        scratch_shapes=[
            pltpu.VMEM((own, half), bf16),
            pltpu.VMEM((ep, own, half), bf16),
            pltpu.VMEM((ep, own, cols), bf16),
            pltpu.VMEM((ep, own, 128), f32),
            pltpu.VMEM((half, cols), bf16),
            pltpu.VMEM((width, hidden), bf16),
            pltpu.VMEM((width, hidden), bf16),
            pltpu.VMEM((hidden, width), bf16),
            pltpu.VMEM((dense, width), bf16),
            pltpu.VMEM((dense, width), bf16),
            pltpu.VMEM((dense, width), bf16),
            pltpu.VMEM((tp, group * own, cols), bf16),
            pltpu.VMEM((group * own, cols), bf16),
            pltpu.VMEM((ep, tp, group * own, cols), bf16),
            pltpu.VMEM((rows, width), bf16),
            pltpu.VMEM((rows, hidden), bf16),
            pltpu.VMEM((rows, dense), bf16),
            pltpu.VMEM((pieces, tp, ep, last, piece), bf16),
            pltpu.VMEM((pieces, ep, last, piece), bf16),
            pltpu.VMEM((pieces, ep, last, piece), bf16),
            pltpu.VMEM((pieces, ep, last, piece), bf16),
            dma((7,)),
            dma((ep,)),
            dma((ep,)),
            dma((ep,)),
            dma((ep,)),
            dma((ep,)),
            dma((ep,)),
            dma,
            dma,
            dma((ep,)),
            dma((ep,)),
            dma((ep,)),
            dma((ep,)),
            dma((pieces,)),
            dma((pieces,)),
            dma((pieces, ep)),
            dma((pieces, ep)),
        ],
        compiler_params=pltpu.CompilerParams(
            collective_id=1, has_side_effects=True, vmem_limit_bytes=56 * 2**20
        ),
        name="experts",
    )(
        read,
        fresh_inputs,
        chosen_specialist.T,
        chosen_coefficient.T,
        row(second_rescale),
        row(common_switch),
        final_projector,
        specialist_switch,
        specialist_expand,
        specialist_contract,
        common_activator.T,
        common_expand.T,
        common_contract,
    )
    return (new_tokens, memory_after)


def solution(mesh):
    placed = (
        P(("grp", "ep"), None),
        P(("grp", "ep"), "tp", None, None),
        P(("grp", "ep"), None),
        P(("grp", "ep"), None),
        P(),
        P(),
        P("tp", "ep"),
        P("tp", "ep"),
        P("tp", "ep"),
        P("tp", "ep"),
        P(),
        P(None, "tp"),
        P("tp"),
        P(),
        P(None, "tp"),
        P("tp"),
        P("tp"),
        P("tp", None),
        P(None, ("ep", "tp")),
        P(None, ("ep", "tp")),
        P(("ep", "tp"), None),
        P(None, ("ep", "tp")),
        P(None, ("ep", "tp")),
        P(("ep", "tp"), None),
        P(),
    )
    return jax.shard_map(
        layer,
        mesh=mesh,
        in_specs=placed,
        out_specs=(P(("grp", "ep", "tp"), None), P(("grp", "ep"), "tp", None, None)),
        check_vma=False,
    )
```

```python
import functools
import math

import jax
import jax.numpy as jnp
from jax import lax
from jax.experimental import pallas as pl
from jax.experimental.pallas import tpu as pltpu
from jax.sharding import PartitionSpec as P

LANE_WIDTH = 64
FF_E = 7168


RMS_EPS = 1e-06
GROUP_EPS = 0.00064
HIGHEST = lax.Precision.HIGHEST
MESH = pl.DeviceIdType.MESH
VMEM_ROOM = 40 * 2**20


def rms_norm(values, norm_gain):
    mean_sq = jnp.mean(values * values, axis=-1, keepdims=True)
    return values * lax.rsqrt(mean_sq + RMS_EPS) * norm_gain


def widen(rounded):
    return lax.optimization_barrier(rounded).astype(jnp.float32)


def evolve_memory(
    memory_arrays,
    receiver_lanes,
    address_lanes,
    content_lanes,
    forget_lanes,
    learning_lanes,
    lane_rescale,
    instant_reward,
):
    unit_key = address_lanes * lax.rsqrt(
        jnp.sum(address_lanes * address_lanes, axis=-1, keepdims=True) + 1.0
    )
    stepped_address = address_lanes * learning_lanes
    removal = jnp.einsum("bhvk,bhk->bhv", memory_arrays, unit_key, precision=HIGHEST)
    memory_after = (
        memory_arrays * forget_lanes[:, :, None, :]
        - removal[..., None] * (unit_key * learning_lanes)[:, :, None, :]
        + content_lanes[..., None] * stepped_address[:, :, None, :]
    )
    memory_retrieval = jnp.einsum("bhvk,bhk->bhv", memory_after, receiver_lanes, precision=HIGHEST)
    centred = memory_retrieval - jnp.mean(memory_retrieval, axis=-1, keepdims=True)
    unit_address = centred * lax.rsqrt(
        jnp.mean(centred * centred, axis=-1, keepdims=True) + GROUP_EPS
    )
    instant_extra = (
        jnp.sum(receiver_lanes * stepped_address * instant_reward, axis=-1, keepdims=True)
        * content_lanes
    )
    return (memory_after, unit_address * lane_rescale + instant_extra)


def swiglu(rows_in, gate_w, up_w):
    gate_val = jnp.dot(rows_in, gate_w, preferred_element_type=jnp.float32)
    up_val = jnp.dot(rows_in, up_w, preferred_element_type=jnp.float32)
    return (jax.nn.silu(gate_val) * up_val).astype(jnp.bfloat16)


def body(
    fresh_inputs,
    memory_arrays,
    chosen_specialist,
    chosen_coefficient,
    first_rescale,
    second_rescale,
    receiver_projector,
    address_projector,
    content_projector,
    final_projector,
    forget_narrowing,
    forget_widening,
    forget_bias,
    learning_narrowing,
    learning_widening,
    learning_bias,
    lane_scaling,
    instant_reward,
    specialist_switch,
    specialist_expand,
    specialist_contract,
    common_activator,
    common_expand,
    common_contract,
    common_switch,
):
    own_rows = fresh_inputs.shape[0]
    model_width = fresh_inputs.shape[1]
    tp_count = lax.axis_size("tp")
    tp_rank = lax.axis_index("tp")
    half_width = model_width // tp_count
    head_count = half_width // LANE_WIDTH
    residual = fresh_inputs.astype(jnp.float32)
    normed = rms_norm(residual, first_rescale).astype(jnp.bfloat16)
    normed_half = lax.dynamic_slice_in_dim(normed, tp_rank * half_width, half_width, 1)
    local_weights = jnp.stack((receiver_projector, address_projector, content_projector), axis=1)
    projected_rows = jnp.einsum(
        "rd,dkc->rkc",
        lax.all_gather(normed_half, "ep", axis=0, tiled=True),
        local_weights,
        preferred_element_type=jnp.float32,
    ).astype(jnp.bfloat16)
    partial_value = lax.all_to_all(projected_rows, "ep", split_axis=0, concat_axis=2, tiled=True)
    projected = lax.psum(widen(partial_value).astype(jnp.bfloat16), "tp")
    mine = lax.dynamic_slice_in_dim(projected, tp_rank * half_width, half_width, 2)

    def divide_lanes(channels):
        return channels.astype(jnp.float32).reshape(own_rows, head_count, LANE_WIDTH)

    decay_mid = jnp.tanh(
        jnp.dot(normed, forget_narrowing, preferred_element_type=jnp.float32)
    ).astype(jnp.bfloat16)
    decay_pre = forget_bias + jnp.dot(
        decay_mid, forget_widening, preferred_element_type=jnp.float32
    )
    decay_vals = jnp.exp(-jnp.exp(-jax.nn.softplus(-decay_pre) - 0.5))
    rate_mid = jnp.dot(normed, learning_narrowing, preferred_element_type=jnp.float32).astype(
        jnp.bfloat16
    )
    rate_vals = jax.nn.sigmoid(
        learning_bias + jnp.dot(rate_mid, learning_widening, preferred_element_type=jnp.float32)
    )
    memory_after, memory_retrieval = evolve_memory(
        memory_arrays,
        divide_lanes(mine[:, 0]),
        divide_lanes(mine[:, 1]),
        divide_lanes(mine[:, 2]),
        divide_lanes(decay_vals),
        divide_lanes(rate_vals),
        lane_scaling.reshape(head_count, LANE_WIDTH),
        instant_reward,
    )
    attended = memory_retrieval.reshape(own_rows, half_width).astype(jnp.bfloat16)
    done_rows = jnp.dot(
        lax.all_gather(attended, "ep", axis=0, tiled=True),
        final_projector,
        preferred_element_type=jnp.float32,
    ).astype(jnp.bfloat16)
    out_part = lax.all_to_all(done_rows, "ep", split_axis=0, concat_axis=1, tiled=True)
    mixed_out = lax.psum(widen(out_part).astype(jnp.bfloat16), "tp")
    residual = residual + mixed_out.astype(jnp.float32)
    ffn_in = rms_norm(residual, second_rescale).astype(jnp.bfloat16)
    all_in, all_weight, all_ids = (
        lax.all_gather(ffn_in, "ep", axis=0, tiled=True),
        lax.all_gather(chosen_coefficient, "ep", axis=0, tiled=True),
        lax.all_gather(chosen_specialist, "ep", axis=0, tiled=True),
    )
    column_count = specialist_switch.shape[1]
    flat_rank = lax.axis_index("ep") * tp_count + tp_rank
    expert = flat_rank * column_count // FF_E
    expert_share = jnp.sum(
        jnp.where(all_ids == expert, all_weight.astype(jnp.float32), 0.0), axis=1
    )
    hidden = swiglu(all_in, specialist_switch, specialist_expand)
    shared_hidden = swiglu(all_in, common_activator, common_expand)
    branch_scale = jax.nn.sigmoid(
        jnp.dot(all_in, common_switch, preferred_element_type=jnp.float32)
    )
    rows_mine = own_rows // tp_count
    expert_term = expert_share[:, None] * jnp.dot(
        hidden, specialist_contract, preferred_element_type=jnp.float32
    )
    routed = lax.psum_scatter(
        expert_term
        + branch_scale[:, None]
        * jnp.dot(shared_hidden, common_contract, preferred_element_type=jnp.float32),
        ("ep", "tp"),
        scatter_dimension=0,
        tiled=True,
    )
    own_residual = lax.dynamic_slice_in_dim(residual, tp_rank * rows_mine, rows_mine, 0)
    return ((own_residual + routed).astype(jnp.bfloat16), memory_after)


def _others(ep, tp, fn):
    me, core = lax.axis_index("ep"), lax.axis_index("tp")
    for far in range(ep):
        for side in range(tp):
            if far or side:
                fn(lax.rem(me + far, ep), lax.rem(core + side, tp))


def _greet(ep, tp):
    barrier = pltpu.get_barrier_semaphore()
    _others(
        ep,
        tp,
        lambda e, t: pl.semaphore_signal(
            barrier, inc=1, device_id={"ep": e, "tp": t}, device_id_type=MESH
        ),
    )


def _met(ep, tp):
    pl.semaphore_wait(pltpu.get_barrier_semaphore(), ep * tp - 1)


def _remote(src, dst, send, recv, e, t):
    return pltpu.make_async_remote_copy(
        src_ref=src,
        dst_ref=dst,
        send_sem=send,
        recv_sem=recv,
        device_id={"ep": e, "tp": t},
        device_id_type=MESH,
    )


def across_dot(left, right):
    return lax.dot_general(
        left, right, (((1,), (1,)), ((), ())), preferred_element_type=jnp.float32
    )


def by_head(ref, channels, first):
    for h in range(channels.shape[1] // LANE_WIDTH):
        ref[:, first + h, :] = channels[:, h * LANE_WIDTH : (h + 1) * LANE_WIDTH]


def split_dot(left, right, dims):
    tops = [f.astype(jnp.bfloat16) for f in (left, right)]
    rests = [(f - h.astype(jnp.float32)).astype(jnp.bfloat16) for f, h in zip((left, right), tops)]
    pairs = ((tops[0], rests[1]), (rests[0], tops[1]), (tops[0], tops[1]))
    return sum(
        lax.dot_general(a, b, (dims, ((), ())), preferred_element_type=jnp.float32)
        for a, b in pairs
    )


def state_kernel(
    memory, query, key, value, decay, rate, lane_gain, reward, after, read, flip, probes, moves
):
    count, heads = query.shape[0], query.shape[1]
    lane = lax.broadcasted_iota(jnp.int32, (LANE_WIDTH, 128), 1)
    turn = lax.rem(lane, heads)
    chunk = math.gcd(heads, 4)

    def sequence(b, carry):
        q, k, v, d, r = query[b], key[b], value[b], decay[b], rate[b]
        unit = k * lax.rsqrt(jnp.sum(k * k, axis=-1, keepdims=True) + 1.0)
        scaled, pulled, seen = k * r, unit * r, d * q
        flip[2 * heads : 3 * heads] = v
        probes[0:heads] = unit
        probes[heads : 2 * heads] = seen
        moves[0:heads] = -pulled
        moves[2 * heads : 3 * heads] = scaled
        value_cols = flip[...].T
        found = jnp.zeros((LANE_WIDTH, 128), jnp.float32)
        for first in range(0, heads, chunk):
            m = memory[b, first : first + chunk]
            sums = split_dot(m.reshape(chunk * LANE_WIDTH, LANE_WIDTH), probes[...], ((1,), (1,)))
            factors = []
            for i in range(chunk):
                both = sums[i * LANE_WIDTH : (i + 1) * LANE_WIDTH]
                both = jnp.where(lane < 2 * heads, both, value_cols)
                factors.append(jnp.where(turn == first + i, both, 0.0))
                found = found + factors[-1]
            change = split_dot(jnp.concatenate(factors, axis=0), moves[...], ((1,), (0,)))
            for i in range(chunk):
                h = first + i
                after[b, h] = m[i] * d[h : h + 1] + change[i * LANE_WIDTH : (i + 1) * LANE_WIDTH]
        rows = found.T
        out = (
            rows[heads : 2 * heads]
            - rows[0:heads] * jnp.sum(pulled * q, axis=-1, keepdims=True)
            + v * jnp.sum(scaled * q, axis=-1, keepdims=True)
        )
        centred = out - jnp.mean(out, axis=-1, keepdims=True)
        level = lax.rsqrt(jnp.mean(centred * centred, axis=-1, keepdims=True) + GROUP_EPS)
        extra = jnp.sum(q * scaled * reward[...], axis=-1, keepdims=True) * v
        read[b] = centred * level * lane_gain[...] + extra
        return carry

    for ref in (flip, probes, moves):
        ref[...] = jnp.zeros_like(ref)
    lax.fori_loop(0, count, sequence, 0)


def project_kernel(
    ep, tp, x, gain, wq, wk, wv, fnar, fwid, fbias, lnar, lwid, lbias, scaling,
    query, key, value, decay, rate, lane_gain,
    halves, rows_all, w, part, got, wsem, ssem, rsem, psem, gsem, lsem,
):
    me, core = lax.axis_index("ep"), lax.axis_index("tp")
    group = ep // tp
    _greet(ep, tp)
    loads = [pltpu.make_async_copy(ref, w.at[i], wsem.at[i]) for i, ref in enumerate((wq, wk, wv))]
    for load in loads:
        load.start()
    own, width = x.shape
    half = width // tp
    values = x[...].astype(jnp.float32)
    normed = (rms_norm(values, gain[...])).astype(jnp.bfloat16)
    for i in range(tp):
        halves[i] = normed[:, i * half : (i + 1) * half]
    _met(ep, tp)
    sends = []
    for far in range(1, ep):
        e = lax.rem(me + far, ep)
        sends.append(
            _remote(halves.at[core], rows_all.at[me], ssem.at[far], rsem.at[me], e, core)
        )
        sends[-1].start()
    rows_all[me] = halves[core]
    decay_mid = jnp.tanh(across_dot(normed, fnar[...])).astype(jnp.bfloat16)
    decay_pre = fbias[...] + jnp.dot(decay_mid, fwid[...], preferred_element_type=jnp.float32)
    by_head(decay, jnp.exp(-(math.exp(-0.5) / (1.0 + jnp.exp(-decay_pre)))), 0)
    rate_mid = across_dot(normed, lnar[...]).astype(jnp.bfloat16)
    rate_pre = lbias[...] + jnp.dot(rate_mid, lwid[...], preferred_element_type=jnp.float32)
    by_head(rate, 1.0 / (1.0 + jnp.exp(-rate_pre)), 0)
    for h in range(lane_gain.shape[0]):
        lane_gain[h : h + 1] = scaling[:, h * LANE_WIDTH : (h + 1) * LANE_WIDTH]
    for load in loads:
        load.wait()
    for far in range(1, ep):
        e = lax.rem(me + far, ep)
        pltpu.make_async_copy(rows_all.at[e], rows_all.at[e], rsem.at[e]).wait()
    every = rows_all[...].reshape(ep * own, half)
    for i in range(3):
        done = jnp.dot(every, w[i], preferred_element_type=jnp.float32)
        part[:, i] = done.astype(jnp.bfloat16).reshape(ep, own, done.shape[1])
    goal = me // group
    slot = core * group + lax.rem(me, group)
    for far in range(1, ep):
        e = lax.rem(me + far, ep)
        _remote(part.at[e], got.at[slot], psem.at[far], gsem.at[slot], e, goal).start()
    here = goal == core
    local = pltpu.make_async_copy(part.at[me], got.at[slot], gsem.at[slot])
    across = _remote(part.at[me], got.at[slot], psem.at[0], gsem.at[slot], me, goal)

    @pl.when(here)
    def _():
        local.start()

    @pl.when(jnp.logical_not(here))
    def _():
        across.start()

    for i in range(ep):
        pltpu.make_async_copy(got.at[i], got.at[i], gsem.at[i]).wait()
    cols = w.shape[2]
    for j in range(group):
        for i in range(3):
            total = got[j, i].astype(jnp.float32)
            for s in range(1, tp):
                total = total + got[s * group + j, i].astype(jnp.float32)
            total = total.astype(jnp.bfloat16).astype(jnp.float32)
            by_head((query, key, value)[i], total, j * (cols // LANE_WIDTH))
    for send in sends:
        send.wait_send()
    for far in range(1, ep):
        _remote(part.at[me], got.at[slot], psem.at[far], gsem.at[slot], me, goal).wait_send()

    @pl.when(jnp.logical_not(here))
    def _():
        across.wait_send()


def ffn_kernel(
    ep, tp, expert_cols, read, x, ids, coef, gain, cs, wo_h, wg_h, wu_h, wd_h, cg_h, cu_h, cd_h,
    out,
    att, att_all, xcol, share, wo, wg, wu, wd, cg, cu, cd, pbuf, psib, res, ffn, hid, chid,
    sibout, sibin, mine, got,
    wsem, s_att, r_att, s_x, r_x, s_sh, r_sh, s_p, r_p, s_res, r_res, f_res, b_res,
    s_sib, r_sib, s_out, r_out,
):
    me, core = lax.axis_index("ep"), lax.axis_index("tp")
    mate = lax.rem(core + 1, tp)
    group = ep // tp
    own, width = x.shape
    cols = wo.shape[1]
    _greet(ep, tp)
    loads = [
        pltpu.make_async_copy(a, b, wsem.at[i])
        for i, (a, b) in enumerate(
            ((wo_h, wo), (wg_h, wg), (wu_h, wu), (cg_h, cg), (cu_h, cu), (wd_h, wd), (cd_h, cd))
        )
    ]
    for load in loads:
        load.start()
    lane = lax.broadcasted_iota(jnp.int32, (own, 128), 1)
    routes = jnp.zeros((own, 128), jnp.float32)
    ids_cols, coef_cols = ids[...].T, coef[...].astype(jnp.float32).T
    for k in range(ids.shape[0]):
        routes = routes + jnp.where(
            ids_cols[:, k : k + 1] == lane, coef_cols[:, k : k + 1], 0.0
        )
    share[me] = routes.astype(jnp.bfloat16)
    pack = 128 // LANE_WIDTH
    for h in range(0, read.shape[1], pack):
        joined = jnp.concatenate([read[:, h + i, :] for i in range(pack)], axis=-1)
        att[:, h * LANE_WIDTH : h * LANE_WIDTH + 128] = joined.astype(jnp.bfloat16)
    _met(ep, tp)
    sends = []

    def push(*args):
        sends.append(_remote(*args))
        sends[-1].start()

    for far in range(1, ep):
        e = lax.rem(me + far, ep)
        push(att, att_all.at[me], s_att.at[far], r_att.at[me], e, core)
    side = me // group
    blocks = []
    for far in range(1, ep):
        e = lax.rem(me + far, ep)
        block = x.at[:, pl.ds(pl.multiple_of(e * cols, cols), cols)]
        blocks.append(_remote(block, xcol.at[me], s_x.at[far], r_x.at[me], e, core))

    @pl.when(side == core)
    def _():
        for copy in blocks:
            copy.start()

    for far in range(1, ep):
        e = lax.rem(me + far, ep)
        push(share.at[me], share.at[me], s_sh.at[far], r_sh.at[me], e, core)
    att_all[me] = att[...]
    xcol[me] = x[:, pl.ds(pl.multiple_of(me * cols, cols), cols)]
    loads[0].wait()

    def arrive(ref, sem):
        pltpu.make_async_copy(ref, ref, sem).wait()

    for far in range(1, ep):
        e = lax.rem(me + far, ep)
        arrive(att_all.at[e], r_att.at[e])
    half = att.shape[1]
    done = jnp.dot(
        att_all[...].reshape(ep * own, half), wo[...], preferred_element_type=jnp.float32
    ).astype(jnp.bfloat16)
    pbuf[...] = done.reshape(tp, group * own, cols)
    push(pbuf.at[mate], psib, s_p, r_p, me, mate)
    for j in range(group):
        e = core * group + j

        @pl.when(e != me)
        def _():
            arrive(xcol.at[e], r_x.at[e])

    arrive(psib, r_p)
    mixed = (pbuf[core].astype(jnp.float32) + psib[...].astype(jnp.float32)).astype(jnp.bfloat16)
    held = xcol[pl.ds(core * group, group)].reshape(group * own, cols).astype(jnp.float32)
    res[me, core] = (held + mixed.astype(jnp.float32)).astype(jnp.bfloat16)
    for far in range(1, ep):
        e = lax.rem(me + far, ep)
        push(res.at[me, core], res.at[me, core], s_res.at[far], r_res.at[me], e, core)
    push(res.at[me, core], res.at[me, core], f_res.at[me], b_res.at[me], me, mate)
    for far in range(1, ep):
        e = lax.rem(me + far, ep)
        arrive(res.at[e, core], r_res.at[e])
        push(res.at[e, core], res.at[e, core], f_res.at[e], b_res.at[e], me, mate)
    for far in range(ep):
        e = lax.rem(me + far, ep)
        arrive(res.at[e, mate], b_res.at[e])
    rows = ep * own
    square = jnp.zeros((rows, 1), jnp.float32)
    for s in range(ep):
        block = res[s].reshape(rows, cols).astype(jnp.float32)
        square = square + jnp.sum(block * block, axis=-1, keepdims=True)
    inv = lax.rsqrt(square / width + RMS_EPS)
    gate_sum = jnp.zeros((rows, 1), jnp.float32)
    for s in range(ep):
        at = slice(s * cols, (s + 1) * cols)
        block = res[s].reshape(rows, cols).astype(jnp.float32)
        block = (block * inv * gain[:, at]).astype(jnp.bfloat16)
        ffn[:, at] = block
        gate_sum = gate_sum + jnp.sum(
            block.astype(jnp.float32) * cs[:, at].astype(jnp.float32), axis=-1, keepdims=True
        )
    branch_scale = 1.0 / (1.0 + jnp.exp(-gate_sum))
    for far in range(1, ep):
        e = lax.rem(me + far, ep)
        arrive(share.at[e], r_sh.at[e])
    expert = (me * tp + core) * wg.shape[1] // expert_cols
    table = share[...].astype(jnp.float32).reshape(rows, 128)
    picked = lax.broadcasted_iota(jnp.int32, (rows, 128), 1) == expert
    weight = jnp.sum(jnp.where(picked, table, 0.0), axis=-1, keepdims=True)
    for i in (1, 2):
        loads[i].wait()

    def widen_up(c, _):
        at = pl.ds(pl.multiple_of(c * 256, 256), 256)
        g = jnp.dot(ffn[...], wg[:, at], preferred_element_type=jnp.float32)
        u = jnp.dot(ffn[...], wu[:, at], preferred_element_type=jnp.float32)
        hid[:, at] = (g / (1.0 + jnp.exp(-g)) * u).astype(jnp.bfloat16)
        return _

    lax.fori_loop(0, wg.shape[1] // 256, widen_up, 0)
    for i in (3, 4):
        loads[i].wait()
    g, u = across_dot(ffn[...], cg[...]), across_dot(ffn[...], cu[...])
    chid[...] = (g / (1.0 + jnp.exp(-g)) * u).astype(jnp.bfloat16)
    for i in (5, 6):
        loads[i].wait()
    pieces = mine.shape[0]
    piece = width // pieces
    last = own // tp
    for n in range(pieces):
        at = slice(n * piece, (n + 1) * piece)
        y = weight * jnp.dot(hid[...], wd[:, at], preferred_element_type=jnp.float32)
        y = y + branch_scale * jnp.dot(chid[...], cd[:, at], preferred_element_type=jnp.float32)
        y = y.reshape(ep, tp, last, piece)
        for k in range(tp):
            sibout[n, k] = y[:, k].astype(jnp.bfloat16)
        push(sibout.at[n, mate], sibin.at[n], s_sib.at[n], r_sib.at[n], me, mate)
    for n in range(pieces):
        arrive(sibin.at[n], r_sib.at[n])
        mine[n] = (
            sibout[n, core].astype(jnp.float32) + sibin[n].astype(jnp.float32)
        ).astype(jnp.bfloat16)
        for far in range(1, ep):
            e = lax.rem(me + far, ep)
            push(mine.at[n, e], got.at[n, me], s_out.at[n, far], r_out.at[n, me], e, core)
    start = pl.multiple_of(lax.rem(me, group) * own, own)
    per = piece // cols
    for n in range(pieces):
        total = mine[n, me].astype(jnp.float32)
        for far in range(1, ep):
            e = lax.rem(me + far, ep)
            arrive(got.at[n, e], r_out.at[n, e])
            total = total + got[n, e].astype(jnp.float32)
        for s in range(per):
            base = res[n * per + s, me // group, pl.ds(start, own)].astype(jnp.float32)
            base = jnp.where(core == 0, base[:last], base[last:])
            a = n * piece + s * cols
            out[:, a : a + cols] = (base + total[:, s * cols : (s + 1) * cols]).astype(jnp.bfloat16)
    for send in sends:
        send.wait_send()

    @pl.when(side == core)
    def _():
        for copy in blocks:
            copy.wait_send()


def layer(*blocks):
    own = blocks[0].shape[0]
    cols, hidden = blocks[9].shape[1], blocks[18].shape[1]
    heads = blocks[17].shape[0]
    tiles = cols % 128 == 0 and hidden % 256 == 0 and own % 16 == 0
    tiles = tiles and heads % 8 == 0 and 128 % heads == 0 and heads <= 32
    heads_match = lax.axis_size("ep") % lax.axis_size("tp") == 0 and lax.axis_size("tp") == 2
    weights = sum(2 * w.size for w in blocks[18:24])
    rows = own * lax.axis_size("ep")
    held = weights + rows * (12 * blocks[0].shape[1] + 8 * hidden)
    small = held < VMEM_ROOM
    return (kernel_body if tiles and heads_match and small else body)(*blocks)


def kernel_body(
    fresh_inputs,
    memory_arrays,
    chosen_specialist,
    chosen_coefficient,
    first_rescale,
    second_rescale,
    receiver_projector,
    address_projector,
    content_projector,
    final_projector,
    forget_narrowing,
    forget_widening,
    forget_bias,
    learning_narrowing,
    learning_widening,
    learning_bias,
    lane_scaling,
    instant_reward,
    specialist_switch,
    specialist_expand,
    specialist_contract,
    common_activator,
    common_expand,
    common_contract,
    common_switch,
):
    ep, tp = lax.axis_size("ep"), lax.axis_size("tp")
    own, width = fresh_inputs.shape
    half, cols = width // tp, final_projector.shape[1]
    heads = half // LANE_WIDTH
    group = ep // tp
    vmem = pl.BlockSpec(memory_space=pltpu.VMEM)
    hbm = pl.BlockSpec(memory_space=pl.ANY)
    bf16, f32 = jnp.bfloat16, jnp.float32
    dma = pltpu.SemaphoreType.DMA

    def row(vector):
        return vector.reshape(1, -1)

    per_head = jax.ShapeDtypeStruct((own, heads, LANE_WIDTH), f32)
    *lanes, lane_gain = pl.pallas_call(
        functools.partial(project_kernel, ep, tp),
        out_shape=(per_head,) * 5 + (jax.ShapeDtypeStruct((heads, LANE_WIDTH), f32),),
        in_specs=[vmem] * 2 + [hbm] * 3 + [vmem] * 7,
        out_specs=(vmem,) * 6,
        scratch_shapes=[
            pltpu.VMEM((tp, own, half), bf16),
            pltpu.VMEM((ep, own, half), bf16),
            pltpu.VMEM((3, half, cols), bf16),
            pltpu.VMEM((ep, 3, own, cols), bf16),
            pltpu.VMEM((ep, 3, own, cols), bf16),
            dma((3,)),
            dma((ep,)),
            dma((ep,)),
            dma((ep,)),
            dma((ep,)),
            dma((1,)),
        ],
        compiler_params=pltpu.CompilerParams(collective_id=0, has_side_effects=True),
        name="project",
    )(
        fresh_inputs,
        row(first_rescale),
        receiver_projector,
        address_projector,
        content_projector,
        forget_narrowing.T,
        forget_widening,
        row(forget_bias),
        learning_narrowing.T,
        learning_widening,
        row(learning_bias),
        row(lane_scaling),
    )
    step = 2
    lane_spec = pl.BlockSpec((step, heads, LANE_WIDTH), lambda i: (i, 0, 0))
    gain_spec = pl.BlockSpec((heads, LANE_WIDTH), lambda i: (0, 0))
    memory_spec = pl.BlockSpec((step, heads, LANE_WIDTH, LANE_WIDTH), lambda i: (i, 0, 0, 0))
    memory_after, read = pl.pallas_call(
        state_kernel,
        grid=(own // step,),
        out_shape=(jax.ShapeDtypeStruct(memory_arrays.shape, f32), per_head),
        in_specs=[memory_spec] + [lane_spec] * 5 + [gain_spec] * 2,
        out_specs=(memory_spec, lane_spec),
        scratch_shapes=[pltpu.VMEM((128, LANE_WIDTH), f32)] * 3,
        name="state",
    )(memory_arrays, *lanes, lane_gain, instant_reward)
    rows, hidden, dense = ep * own, specialist_switch.shape[1], common_activator.shape[1]
    pieces = 4
    piece, last = width // pieces, own // tp
    new_tokens = pl.pallas_call(
        functools.partial(ffn_kernel, ep, tp, FF_E),
        out_shape=jax.ShapeDtypeStruct((last, width), bf16),
        in_specs=[vmem] * 6 + [hbm] * 7,
        out_specs=vmem,
        scratch_shapes=[
            pltpu.VMEM((own, half), bf16),
            pltpu.VMEM((ep, own, half), bf16),
            pltpu.VMEM((ep, own, cols), bf16),
            pltpu.VMEM((ep, own, 128), bf16),
            pltpu.VMEM((half, cols), bf16),
            pltpu.VMEM((width, hidden), bf16),
            pltpu.VMEM((width, hidden), bf16),
            pltpu.VMEM((hidden, width), bf16),
            pltpu.VMEM((dense, width), bf16),
            pltpu.VMEM((dense, width), bf16),
            pltpu.VMEM((dense, width), bf16),
            pltpu.VMEM((tp, group * own, cols), bf16),
            pltpu.VMEM((group * own, cols), bf16),
            pltpu.VMEM((ep, tp, group * own, cols), bf16),
            pltpu.VMEM((rows, width), bf16),
            pltpu.VMEM((rows, hidden), bf16),
            pltpu.VMEM((rows, dense), bf16),
            pltpu.VMEM((pieces, tp, ep, last, piece), bf16),
            pltpu.VMEM((pieces, ep, last, piece), bf16),
            pltpu.VMEM((pieces, ep, last, piece), bf16),
            pltpu.VMEM((pieces, ep, last, piece), bf16),
            dma((7,)),
            dma((ep,)),
            dma((ep,)),
            dma((ep,)),
            dma((ep,)),
            dma((ep,)),
            dma((ep,)),
            dma,
            dma,
            dma((ep,)),
            dma((ep,)),
            dma((ep,)),
            dma((ep,)),
            dma((pieces,)),
            dma((pieces,)),
            dma((pieces, ep)),
            dma((pieces, ep)),
        ],
        compiler_params=pltpu.CompilerParams(
            collective_id=1, has_side_effects=True, vmem_limit_bytes=56 * 2**20
        ),
        name="experts",
    )(
        read,
        fresh_inputs,
        chosen_specialist.T,
        chosen_coefficient.T,
        row(second_rescale),
        row(common_switch),
        final_projector,
        specialist_switch,
        specialist_expand,
        specialist_contract,
        common_activator.T,
        common_expand.T,
        common_contract,
    )
    return (new_tokens, memory_after)


def solution(mesh):
    placed = (
        P(("grp", "ep"), None),
        P(("grp", "ep"), "tp", None, None),
        P(("grp", "ep"), None),
        P(("grp", "ep"), None),
        P(),
        P(),
        P("tp", "ep"),
        P("tp", "ep"),
        P("tp", "ep"),
        P("tp", "ep"),
        P(),
        P(None, "tp"),
        P("tp"),
        P(),
        P(None, "tp"),
        P("tp"),
        P("tp"),
        P("tp", None),
        P(None, ("ep", "tp")),
        P(None, ("ep", "tp")),
        P(("ep", "tp"), None),
        P(None, ("ep", "tp")),
        P(None, ("ep", "tp")),
        P(("ep", "tp"), None),
        P(),
    )
    return jax.shard_map(
        layer,
        mesh=mesh,
        in_specs=placed,
        out_specs=(P(("grp", "ep", "tp"), None), P(("grp", "ep"), "tp", None, None)),
        check_vma=False,
    )
```

```python
import functools
import math

import jax
import jax.numpy as jnp
from jax import lax
from jax.experimental import pallas as pl
from jax.experimental.pallas import tpu as pltpu
from jax.sharding import PartitionSpec as P

LANE_WIDTH = 64
FF_E = 7168


RMS_EPS = 1e-06
GROUP_EPS = 0.00064
HIGHEST = lax.Precision.HIGHEST
MESH = pl.DeviceIdType.MESH
VMEM_ROOM = 40 * 2**20


def rms_norm(values, norm_gain):
    mean_sq = jnp.mean(values * values, axis=-1, keepdims=True)
    return values * lax.rsqrt(mean_sq + RMS_EPS) * norm_gain


def widen(rounded):
    return lax.optimization_barrier(rounded).astype(jnp.float32)


def evolve_memory(
    memory_arrays,
    receiver_lanes,
    address_lanes,
    content_lanes,
    forget_lanes,
    learning_lanes,
    lane_rescale,
    instant_reward,
):
    unit_key = address_lanes * lax.rsqrt(
        jnp.sum(address_lanes * address_lanes, axis=-1, keepdims=True) + 1.0
    )
    stepped_address = address_lanes * learning_lanes
    removal = jnp.einsum("bhvk,bhk->bhv", memory_arrays, unit_key, precision=HIGHEST)
    memory_after = (
        memory_arrays * forget_lanes[:, :, None, :]
        - removal[..., None] * (unit_key * learning_lanes)[:, :, None, :]
        + content_lanes[..., None] * stepped_address[:, :, None, :]
    )
    memory_retrieval = jnp.einsum("bhvk,bhk->bhv", memory_after, receiver_lanes, precision=HIGHEST)
    centred = memory_retrieval - jnp.mean(memory_retrieval, axis=-1, keepdims=True)
    unit_address = centred * lax.rsqrt(
        jnp.mean(centred * centred, axis=-1, keepdims=True) + GROUP_EPS
    )
    instant_extra = (
        jnp.sum(receiver_lanes * stepped_address * instant_reward, axis=-1, keepdims=True)
        * content_lanes
    )
    return (memory_after, unit_address * lane_rescale + instant_extra)


def swiglu(rows_in, gate_w, up_w):
    gate_val = jnp.dot(rows_in, gate_w, preferred_element_type=jnp.float32)
    up_val = jnp.dot(rows_in, up_w, preferred_element_type=jnp.float32)
    return (jax.nn.silu(gate_val) * up_val).astype(jnp.bfloat16)


def body(
    fresh_inputs,
    memory_arrays,
    chosen_specialist,
    chosen_coefficient,
    first_rescale,
    second_rescale,
    receiver_projector,
    address_projector,
    content_projector,
    final_projector,
    forget_narrowing,
    forget_widening,
    forget_bias,
    learning_narrowing,
    learning_widening,
    learning_bias,
    lane_scaling,
    instant_reward,
    specialist_switch,
    specialist_expand,
    specialist_contract,
    common_activator,
    common_expand,
    common_contract,
    common_switch,
):
    own_rows = fresh_inputs.shape[0]
    model_width = fresh_inputs.shape[1]
    tp_count = lax.axis_size("tp")
    tp_rank = lax.axis_index("tp")
    half_width = model_width // tp_count
    head_count = half_width // LANE_WIDTH
    residual = fresh_inputs.astype(jnp.float32)
    normed = rms_norm(residual, first_rescale).astype(jnp.bfloat16)
    normed_half = lax.dynamic_slice_in_dim(normed, tp_rank * half_width, half_width, 1)
    local_weights = jnp.stack((receiver_projector, address_projector, content_projector), axis=1)
    projected_rows = jnp.einsum(
        "rd,dkc->rkc",
        lax.all_gather(normed_half, "ep", axis=0, tiled=True),
        local_weights,
        preferred_element_type=jnp.float32,
    ).astype(jnp.bfloat16)
    partial_value = lax.all_to_all(projected_rows, "ep", split_axis=0, concat_axis=2, tiled=True)
    projected = lax.psum(widen(partial_value).astype(jnp.bfloat16), "tp")
    mine = lax.dynamic_slice_in_dim(projected, tp_rank * half_width, half_width, 2)

    def divide_lanes(channels):
        return channels.astype(jnp.float32).reshape(own_rows, head_count, LANE_WIDTH)

    decay_mid = jnp.tanh(
        jnp.dot(normed, forget_narrowing, preferred_element_type=jnp.float32)
    ).astype(jnp.bfloat16)
    decay_pre = forget_bias + jnp.dot(
        decay_mid, forget_widening, preferred_element_type=jnp.float32
    )
    decay_vals = jnp.exp(-jnp.exp(-jax.nn.softplus(-decay_pre) - 0.5))
    rate_mid = jnp.dot(normed, learning_narrowing, preferred_element_type=jnp.float32).astype(
        jnp.bfloat16
    )
    rate_vals = jax.nn.sigmoid(
        learning_bias + jnp.dot(rate_mid, learning_widening, preferred_element_type=jnp.float32)
    )
    memory_after, memory_retrieval = evolve_memory(
        memory_arrays,
        divide_lanes(mine[:, 0]),
        divide_lanes(mine[:, 1]),
        divide_lanes(mine[:, 2]),
        divide_lanes(decay_vals),
        divide_lanes(rate_vals),
        lane_scaling.reshape(head_count, LANE_WIDTH),
        instant_reward,
    )
    attended = memory_retrieval.reshape(own_rows, half_width).astype(jnp.bfloat16)
    done_rows = jnp.dot(
        lax.all_gather(attended, "ep", axis=0, tiled=True),
        final_projector,
        preferred_element_type=jnp.float32,
    ).astype(jnp.bfloat16)
    out_part = lax.all_to_all(done_rows, "ep", split_axis=0, concat_axis=1, tiled=True)
    mixed_out = lax.psum(widen(out_part).astype(jnp.bfloat16), "tp")
    residual = residual + mixed_out.astype(jnp.float32)
    ffn_in = rms_norm(residual, second_rescale).astype(jnp.bfloat16)
    all_in, all_weight, all_ids = (
        lax.all_gather(ffn_in, "ep", axis=0, tiled=True),
        lax.all_gather(chosen_coefficient, "ep", axis=0, tiled=True),
        lax.all_gather(chosen_specialist, "ep", axis=0, tiled=True),
    )
    column_count = specialist_switch.shape[1]
    flat_rank = lax.axis_index("ep") * tp_count + tp_rank
    expert = flat_rank * column_count // FF_E
    expert_share = jnp.sum(
        jnp.where(all_ids == expert, all_weight.astype(jnp.float32), 0.0), axis=1
    )
    hidden = swiglu(all_in, specialist_switch, specialist_expand)
    shared_hidden = swiglu(all_in, common_activator, common_expand)
    branch_scale = jax.nn.sigmoid(
        jnp.dot(all_in, common_switch, preferred_element_type=jnp.float32)
    )
    rows_mine = own_rows // tp_count
    expert_term = expert_share[:, None] * jnp.dot(
        hidden, specialist_contract, preferred_element_type=jnp.float32
    )
    routed = lax.psum_scatter(
        expert_term
        + branch_scale[:, None]
        * jnp.dot(shared_hidden, common_contract, preferred_element_type=jnp.float32),
        ("ep", "tp"),
        scatter_dimension=0,
        tiled=True,
    )
    own_residual = lax.dynamic_slice_in_dim(residual, tp_rank * rows_mine, rows_mine, 0)
    return ((own_residual + routed).astype(jnp.bfloat16), memory_after)


def _others(ep, tp, fn):
    me, core = lax.axis_index("ep"), lax.axis_index("tp")
    for far in range(ep):
        for side in range(tp):
            if far or side:
                fn(lax.rem(me + far, ep), lax.rem(core + side, tp))


def _greet(ep, tp):
    barrier = pltpu.get_barrier_semaphore()
    _others(
        ep,
        tp,
        lambda e, t: pl.semaphore_signal(
            barrier, inc=1, device_id={"ep": e, "tp": t}, device_id_type=MESH
        ),
    )


def _met(ep, tp):
    pl.semaphore_wait(pltpu.get_barrier_semaphore(), ep * tp - 1)


def _remote(src, dst, send, recv, e, t):
    return pltpu.make_async_remote_copy(
        src_ref=src,
        dst_ref=dst,
        send_sem=send,
        recv_sem=recv,
        device_id={"ep": e, "tp": t},
        device_id_type=MESH,
    )


def across_dot(left, right):
    return lax.dot_general(
        left, right, (((1,), (1,)), ((), ())), preferred_element_type=jnp.float32
    )


def by_head(ref, channels, first):
    for h in range(channels.shape[1] // LANE_WIDTH):
        ref[:, first + h, :] = channels[:, h * LANE_WIDTH : (h + 1) * LANE_WIDTH]


def round_dot(left, right, dims):
    return lax.dot_general(
        left.astype(jnp.bfloat16),
        right.astype(jnp.bfloat16),
        (dims, ((), ())),
        preferred_element_type=jnp.float32,
    )


def state_kernel(
    memory, query, key, value, decay, rate, lane_gain, reward, after, read, flip, probes, moves
):
    count, heads = query.shape[0], query.shape[1]
    lane = lax.broadcasted_iota(jnp.int32, (LANE_WIDTH, 128), 1)
    turn = lax.rem(lane, heads)
    chunk = math.gcd(heads, 4)

    def sequence(b):
        q, k, v, d, r = query[b], key[b], value[b], decay[b], rate[b]
        unit = k * lax.rsqrt(jnp.sum(k * k, axis=-1, keepdims=True) + 1.0)
        scaled, pulled, seen = k * r, unit * r, d * q
        flip[b, 2 * heads : 3 * heads] = v
        probes[b, 0:heads] = unit
        probes[b, heads : 2 * heads] = seen
        moves[b, 0:heads] = -pulled
        moves[b, 2 * heads : 3 * heads] = scaled
        value_cols = flip[b].T
        found = jnp.zeros((LANE_WIDTH, 128), jnp.float32)
        for first in range(0, heads, chunk):
            m = memory[b, first : first + chunk]
            sums = round_dot(m.reshape(chunk * LANE_WIDTH, LANE_WIDTH), probes[b], ((1,), (1,)))
            factors = []
            for i in range(chunk):
                both = sums[i * LANE_WIDTH : (i + 1) * LANE_WIDTH]
                both = jnp.where(lane < 2 * heads, both, value_cols)
                factors.append(jnp.where(turn == first + i, both, 0.0))
                found = found + factors[-1]
            change = round_dot(jnp.concatenate(factors, axis=0), moves[b], ((1,), (0,)))
            for i in range(chunk):
                h = first + i
                after[b, h] = m[i] * d[h : h + 1] + change[i * LANE_WIDTH : (i + 1) * LANE_WIDTH]
        rows = found.T
        out = (
            rows[heads : 2 * heads]
            - rows[0:heads] * jnp.sum(pulled * q, axis=-1, keepdims=True)
            + v * jnp.sum(scaled * q, axis=-1, keepdims=True)
        )
        centred = out - jnp.mean(out, axis=-1, keepdims=True)
        level = lax.rsqrt(jnp.mean(centred * centred, axis=-1, keepdims=True) + GROUP_EPS)
        extra = jnp.sum(q * scaled * reward[...], axis=-1, keepdims=True) * v
        read[b] = centred * level * lane_gain[...] + extra

    for ref in (flip, probes, moves):
        ref[...] = jnp.zeros_like(ref)
    for b in range(count):
        sequence(b)


def project_kernel(
    ep, tp, x, gain, wq, wk, wv, fnar, fwid, fbias, lnar, lwid, lbias, scaling,
    query, key, value, decay, rate, lane_gain,
    halves, rows_all, w, part, got, wsem, ssem, rsem, psem, gsem, lsem,
):
    me, core = lax.axis_index("ep"), lax.axis_index("tp")
    group = ep // tp
    _greet(ep, tp)
    loads = [pltpu.make_async_copy(ref, w.at[i], wsem.at[i]) for i, ref in enumerate((wq, wk, wv))]
    for load in loads:
        load.start()
    own, width = x.shape
    half = width // tp
    values = x[...].astype(jnp.float32)
    normed = (rms_norm(values, gain[...])).astype(jnp.bfloat16)
    for i in range(tp):
        halves[i] = normed[:, i * half : (i + 1) * half]
    _met(ep, tp)
    sends = []
    for far in range(1, ep):
        e = lax.rem(me + far, ep)
        sends.append(
            _remote(halves.at[core], rows_all.at[me], ssem.at[far], rsem.at[me], e, core)
        )
        sends[-1].start()
    rows_all[me] = halves[core]
    decay_mid = jnp.tanh(across_dot(normed, fnar[...])).astype(jnp.bfloat16)
    decay_pre = fbias[...] + jnp.dot(decay_mid, fwid[...], preferred_element_type=jnp.float32)
    by_head(decay, jnp.exp(-(math.exp(-0.5) / (1.0 + jnp.exp(-decay_pre)))), 0)
    rate_mid = across_dot(normed, lnar[...]).astype(jnp.bfloat16)
    rate_pre = lbias[...] + jnp.dot(rate_mid, lwid[...], preferred_element_type=jnp.float32)
    by_head(rate, 1.0 / (1.0 + jnp.exp(-rate_pre)), 0)
    for h in range(lane_gain.shape[0]):
        lane_gain[h : h + 1] = scaling[:, h * LANE_WIDTH : (h + 1) * LANE_WIDTH]
    for load in loads:
        load.wait()
    for far in range(1, ep):
        e = lax.rem(me + far, ep)
        pltpu.make_async_copy(rows_all.at[e], rows_all.at[e], rsem.at[e]).wait()
    every = rows_all[...].reshape(ep * own, half)
    for i in range(3):
        done = jnp.dot(every, w[i], preferred_element_type=jnp.float32)
        part[:, i] = done.astype(jnp.bfloat16).reshape(ep, own, done.shape[1])
    goal = me // group
    slot = core * group + lax.rem(me, group)
    for far in range(1, ep):
        e = lax.rem(me + far, ep)
        _remote(part.at[e], got.at[slot], psem.at[far], gsem.at[slot], e, goal).start()
    here = goal == core
    local = pltpu.make_async_copy(part.at[me], got.at[slot], gsem.at[slot])
    across = _remote(part.at[me], got.at[slot], psem.at[0], gsem.at[slot], me, goal)

    @pl.when(here)
    def _():
        local.start()

    @pl.when(jnp.logical_not(here))
    def _():
        across.start()

    for i in range(ep):
        pltpu.make_async_copy(got.at[i], got.at[i], gsem.at[i]).wait()
    cols = w.shape[2]
    for j in range(group):
        for i in range(3):
            total = got[j, i].astype(jnp.float32)
            for s in range(1, tp):
                total = total + got[s * group + j, i].astype(jnp.float32)
            total = total.astype(jnp.bfloat16).astype(jnp.float32)
            by_head((query, key, value)[i], total, j * (cols // LANE_WIDTH))
    for send in sends:
        send.wait_send()
    for far in range(1, ep):
        _remote(part.at[me], got.at[slot], psem.at[far], gsem.at[slot], me, goal).wait_send()

    @pl.when(jnp.logical_not(here))
    def _():
        across.wait_send()


def ffn_kernel(
    ep, tp, expert_cols, read, x, ids, coef, gain, cs, wo_h, wg_h, wu_h, wd_h, cg_h, cu_h, cd_h,
    out,
    att, att_all, xcol, share, wo, wg, wu, wd, cg, cu, cd, pbuf, psib, res, ffn, hid, chid,
    sibout, sibin, mine, got,
    wsem, s_att, r_att, s_x, r_x, s_sh, r_sh, s_p, r_p, s_res, r_res, f_res, b_res,
    s_sib, r_sib, s_out, r_out,
):
    me, core = lax.axis_index("ep"), lax.axis_index("tp")
    mate = lax.rem(core + 1, tp)
    group = ep // tp
    own, width = x.shape
    cols = wo.shape[1]
    _greet(ep, tp)
    loads = [
        pltpu.make_async_copy(a, b, wsem.at[i])
        for i, (a, b) in enumerate(
            ((wo_h, wo), (wg_h, wg), (wu_h, wu), (cg_h, cg), (cu_h, cu), (wd_h, wd), (cd_h, cd))
        )
    ]
    for load in loads:
        load.start()
    lane = lax.broadcasted_iota(jnp.int32, (own, 128), 1)
    routes = jnp.zeros((own, 128), jnp.float32)
    ids_cols, coef_cols = ids[...].T, coef[...].astype(jnp.float32).T
    for k in range(ids.shape[0]):
        routes = routes + jnp.where(
            ids_cols[:, k : k + 1] == lane, coef_cols[:, k : k + 1], 0.0
        )
    share[me] = routes.astype(jnp.bfloat16)
    pack = 128 // LANE_WIDTH
    for h in range(0, read.shape[1], pack):
        joined = jnp.concatenate([read[:, h + i, :] for i in range(pack)], axis=-1)
        att[:, h * LANE_WIDTH : h * LANE_WIDTH + 128] = joined.astype(jnp.bfloat16)
    _met(ep, tp)
    sends = []

    def push(*args):
        sends.append(_remote(*args))
        sends[-1].start()

    for far in range(1, ep):
        e = lax.rem(me + far, ep)
        push(att, att_all.at[me], s_att.at[far], r_att.at[me], e, core)
    side = me // group
    blocks = []
    for far in range(1, ep):
        e = lax.rem(me + far, ep)
        block = x.at[:, pl.ds(pl.multiple_of(e * cols, cols), cols)]
        blocks.append(_remote(block, xcol.at[me], s_x.at[far], r_x.at[me], e, core))

    @pl.when(side == core)
    def _():
        for copy in blocks:
            copy.start()

    for far in range(1, ep):
        e = lax.rem(me + far, ep)
        push(share.at[me], share.at[me], s_sh.at[far], r_sh.at[me], e, core)
    att_all[me] = att[...]
    xcol[me] = x[:, pl.ds(pl.multiple_of(me * cols, cols), cols)]
    loads[0].wait()

    def arrive(ref, sem):
        pltpu.make_async_copy(ref, ref, sem).wait()

    for far in range(1, ep):
        e = lax.rem(me + far, ep)
        arrive(att_all.at[e], r_att.at[e])
    half = att.shape[1]
    done = jnp.dot(
        att_all[...].reshape(ep * own, half), wo[...], preferred_element_type=jnp.float32
    ).astype(jnp.bfloat16)
    pbuf[...] = done.reshape(tp, group * own, cols)
    push(pbuf.at[mate], psib, s_p, r_p, me, mate)
    for j in range(group):
        e = core * group + j

        @pl.when(e != me)
        def _():
            arrive(xcol.at[e], r_x.at[e])

    arrive(psib, r_p)
    mixed = (pbuf[core].astype(jnp.float32) + psib[...].astype(jnp.float32)).astype(jnp.bfloat16)
    held = xcol[pl.ds(core * group, group)].reshape(group * own, cols).astype(jnp.float32)
    res[me, core] = (held + mixed.astype(jnp.float32)).astype(jnp.bfloat16)
    for far in range(1, ep):
        e = lax.rem(me + far, ep)
        push(res.at[me, core], res.at[me, core], s_res.at[far], r_res.at[me], e, core)
    push(res.at[me, core], res.at[me, core], f_res.at[me], b_res.at[me], me, mate)
    for far in range(1, ep):
        e = lax.rem(me + far, ep)
        arrive(res.at[e, core], r_res.at[e])
        push(res.at[e, core], res.at[e, core], f_res.at[e], b_res.at[e], me, mate)
    for far in range(ep):
        e = lax.rem(me + far, ep)
        arrive(res.at[e, mate], b_res.at[e])
    rows = ep * own
    square = jnp.zeros((rows, 1), jnp.float32)
    for s in range(ep):
        block = res[s].reshape(rows, cols).astype(jnp.float32)
        square = square + jnp.sum(block * block, axis=-1, keepdims=True)
    inv = lax.rsqrt(square / width + RMS_EPS)
    gate_sum = jnp.zeros((rows, 1), jnp.float32)
    for s in range(ep):
        at = slice(s * cols, (s + 1) * cols)
        block = res[s].reshape(rows, cols).astype(jnp.float32)
        block = (block * inv * gain[:, at]).astype(jnp.bfloat16)
        ffn[:, at] = block
        gate_sum = gate_sum + jnp.sum(
            block.astype(jnp.float32) * cs[:, at].astype(jnp.float32), axis=-1, keepdims=True
        )
    branch_scale = 1.0 / (1.0 + jnp.exp(-gate_sum))
    for far in range(1, ep):
        e = lax.rem(me + far, ep)
        arrive(share.at[e], r_sh.at[e])
    expert = (me * tp + core) * wg.shape[1] // expert_cols
    table = share[...].astype(jnp.float32).reshape(rows, 128)
    picked = lax.broadcasted_iota(jnp.int32, (rows, 128), 1) == expert
    weight = jnp.sum(jnp.where(picked, table, 0.0), axis=-1, keepdims=True)
    for i in (1, 2):
        loads[i].wait()

    def widen_up(c, _):
        at = pl.ds(pl.multiple_of(c * 256, 256), 256)
        g = jnp.dot(ffn[...], wg[:, at], preferred_element_type=jnp.float32)
        u = jnp.dot(ffn[...], wu[:, at], preferred_element_type=jnp.float32)
        hid[:, at] = (g / (1.0 + jnp.exp(-g)) * u).astype(jnp.bfloat16)
        return _

    lax.fori_loop(0, wg.shape[1] // 256, widen_up, 0)
    for i in (3, 4):
        loads[i].wait()
    g, u = across_dot(ffn[...], cg[...]), across_dot(ffn[...], cu[...])
    chid[...] = (g / (1.0 + jnp.exp(-g)) * u).astype(jnp.bfloat16)
    for i in (5, 6):
        loads[i].wait()
    pieces = mine.shape[0]
    piece = width // pieces
    last = own // tp
    for n in range(pieces):
        at = slice(n * piece, (n + 1) * piece)
        y = weight * jnp.dot(hid[...], wd[:, at], preferred_element_type=jnp.float32)
        y = y + branch_scale * jnp.dot(chid[...], cd[:, at], preferred_element_type=jnp.float32)
        y = y.reshape(ep, tp, last, piece)
        for k in range(tp):
            sibout[n, k] = y[:, k].astype(jnp.bfloat16)
        push(sibout.at[n, mate], sibin.at[n], s_sib.at[n], r_sib.at[n], me, mate)
    for n in range(pieces):
        arrive(sibin.at[n], r_sib.at[n])
        mine[n] = (
            sibout[n, core].astype(jnp.float32) + sibin[n].astype(jnp.float32)
        ).astype(jnp.bfloat16)
        for far in range(1, ep):
            e = lax.rem(me + far, ep)
            push(mine.at[n, e], got.at[n, me], s_out.at[n, far], r_out.at[n, me], e, core)
    start = pl.multiple_of(lax.rem(me, group) * own, own)
    per = piece // cols
    for n in range(pieces):
        total = mine[n, me].astype(jnp.float32)
        for far in range(1, ep):
            e = lax.rem(me + far, ep)
            arrive(got.at[n, e], r_out.at[n, e])
            total = total + got[n, e].astype(jnp.float32)
        for s in range(per):
            base = res[n * per + s, me // group, pl.ds(start, own)].astype(jnp.float32)
            base = jnp.where(core == 0, base[:last], base[last:])
            a = n * piece + s * cols
            out[:, a : a + cols] = (base + total[:, s * cols : (s + 1) * cols]).astype(jnp.bfloat16)
    for send in sends:
        send.wait_send()

    @pl.when(side == core)
    def _():
        for copy in blocks:
            copy.wait_send()


def layer(*blocks):
    own = blocks[0].shape[0]
    cols, hidden = blocks[9].shape[1], blocks[18].shape[1]
    heads = blocks[17].shape[0]
    tiles = cols % 128 == 0 and hidden % 256 == 0 and own % 16 == 0
    tiles = tiles and heads % 8 == 0 and 128 % heads == 0 and heads <= 32
    heads_match = lax.axis_size("ep") % lax.axis_size("tp") == 0 and lax.axis_size("tp") == 2
    weights = sum(2 * w.size for w in blocks[18:24])
    rows = own * lax.axis_size("ep")
    held = weights + rows * (12 * blocks[0].shape[1] + 8 * hidden)
    small = held < VMEM_ROOM
    return (kernel_body if tiles and heads_match and small else body)(*blocks)


def kernel_body(
    fresh_inputs,
    memory_arrays,
    chosen_specialist,
    chosen_coefficient,
    first_rescale,
    second_rescale,
    receiver_projector,
    address_projector,
    content_projector,
    final_projector,
    forget_narrowing,
    forget_widening,
    forget_bias,
    learning_narrowing,
    learning_widening,
    learning_bias,
    lane_scaling,
    instant_reward,
    specialist_switch,
    specialist_expand,
    specialist_contract,
    common_activator,
    common_expand,
    common_contract,
    common_switch,
):
    ep, tp = lax.axis_size("ep"), lax.axis_size("tp")
    own, width = fresh_inputs.shape
    half, cols = width // tp, final_projector.shape[1]
    heads = half // LANE_WIDTH
    group = ep // tp
    vmem = pl.BlockSpec(memory_space=pltpu.VMEM)
    hbm = pl.BlockSpec(memory_space=pl.ANY)
    bf16, f32 = jnp.bfloat16, jnp.float32
    dma = pltpu.SemaphoreType.DMA

    def row(vector):
        return vector.reshape(1, -1)

    per_head = jax.ShapeDtypeStruct((own, heads, LANE_WIDTH), f32)
    *lanes, lane_gain = pl.pallas_call(
        functools.partial(project_kernel, ep, tp),
        out_shape=(per_head,) * 5 + (jax.ShapeDtypeStruct((heads, LANE_WIDTH), f32),),
        in_specs=[vmem] * 2 + [hbm] * 3 + [vmem] * 7,
        out_specs=(vmem,) * 6,
        scratch_shapes=[
            pltpu.VMEM((tp, own, half), bf16),
            pltpu.VMEM((ep, own, half), bf16),
            pltpu.VMEM((3, half, cols), bf16),
            pltpu.VMEM((ep, 3, own, cols), bf16),
            pltpu.VMEM((ep, 3, own, cols), bf16),
            dma((3,)),
            dma((ep,)),
            dma((ep,)),
            dma((ep,)),
            dma((ep,)),
            dma((1,)),
        ],
        compiler_params=pltpu.CompilerParams(collective_id=0, has_side_effects=True),
        name="project",
    )(
        fresh_inputs,
        row(first_rescale),
        receiver_projector,
        address_projector,
        content_projector,
        forget_narrowing.T,
        forget_widening,
        row(forget_bias),
        learning_narrowing.T,
        learning_widening,
        row(learning_bias),
        row(lane_scaling),
    )
    step = 2
    lane_spec = pl.BlockSpec((step, heads, LANE_WIDTH), lambda i: (i, 0, 0))
    gain_spec = pl.BlockSpec((heads, LANE_WIDTH), lambda i: (0, 0))
    memory_spec = pl.BlockSpec((step, heads, LANE_WIDTH, LANE_WIDTH), lambda i: (i, 0, 0, 0))
    memory_after, read = pl.pallas_call(
        state_kernel,
        grid=(own // step,),
        out_shape=(jax.ShapeDtypeStruct(memory_arrays.shape, f32), per_head),
        in_specs=[memory_spec] + [lane_spec] * 5 + [gain_spec] * 2,
        out_specs=(memory_spec, lane_spec),
        scratch_shapes=[pltpu.VMEM((step, 128, LANE_WIDTH), f32)] * 3,
        name="state",
    )(memory_arrays, *lanes, lane_gain, instant_reward)
    rows, hidden, dense = ep * own, specialist_switch.shape[1], common_activator.shape[1]
    pieces = 4
    piece, last = width // pieces, own // tp
    new_tokens = pl.pallas_call(
        functools.partial(ffn_kernel, ep, tp, FF_E),
        out_shape=jax.ShapeDtypeStruct((last, width), bf16),
        in_specs=[vmem] * 6 + [hbm] * 7,
        out_specs=vmem,
        scratch_shapes=[
            pltpu.VMEM((own, half), bf16),
            pltpu.VMEM((ep, own, half), bf16),
            pltpu.VMEM((ep, own, cols), bf16),
            pltpu.VMEM((ep, own, 128), bf16),
            pltpu.VMEM((half, cols), bf16),
            pltpu.VMEM((width, hidden), bf16),
            pltpu.VMEM((width, hidden), bf16),
            pltpu.VMEM((hidden, width), bf16),
            pltpu.VMEM((dense, width), bf16),
            pltpu.VMEM((dense, width), bf16),
            pltpu.VMEM((dense, width), bf16),
            pltpu.VMEM((tp, group * own, cols), bf16),
            pltpu.VMEM((group * own, cols), bf16),
            pltpu.VMEM((ep, tp, group * own, cols), bf16),
            pltpu.VMEM((rows, width), bf16),
            pltpu.VMEM((rows, hidden), bf16),
            pltpu.VMEM((rows, dense), bf16),
            pltpu.VMEM((pieces, tp, ep, last, piece), bf16),
            pltpu.VMEM((pieces, ep, last, piece), bf16),
            pltpu.VMEM((pieces, ep, last, piece), bf16),
            pltpu.VMEM((pieces, ep, last, piece), bf16),
            dma((7,)),
            dma((ep,)),
            dma((ep,)),
            dma((ep,)),
            dma((ep,)),
            dma((ep,)),
            dma((ep,)),
            dma,
            dma,
            dma((ep,)),
            dma((ep,)),
            dma((ep,)),
            dma((ep,)),
            dma((pieces,)),
            dma((pieces,)),
            dma((pieces, ep)),
            dma((pieces, ep)),
        ],
        compiler_params=pltpu.CompilerParams(
            collective_id=1, has_side_effects=True, vmem_limit_bytes=56 * 2**20
        ),
        name="experts",
    )(
        read,
        fresh_inputs,
        chosen_specialist.T,
        chosen_coefficient.T,
        row(second_rescale),
        row(common_switch),
        final_projector,
        specialist_switch,
        specialist_expand,
        specialist_contract,
        common_activator.T,
        common_expand.T,
        common_contract,
    )
    return (new_tokens, memory_after)


def solution(mesh):
    placed = (
        P(("grp", "ep"), None),
        P(("grp", "ep"), "tp", None, None),
        P(("grp", "ep"), None),
        P(("grp", "ep"), None),
        P(),
        P(),
        P("tp", "ep"),
        P("tp", "ep"),
        P("tp", "ep"),
        P("tp", "ep"),
        P(),
        P(None, "tp"),
        P("tp"),
        P(),
        P(None, "tp"),
        P("tp"),
        P("tp"),
        P("tp", None),
        P(None, ("ep", "tp")),
        P(None, ("ep", "tp")),
        P(("ep", "tp"), None),
        P(None, ("ep", "tp")),
        P(None, ("ep", "tp")),
        P(("ep", "tp"), None),
        P(),
    )
    return jax.shard_map(
        layer,
        mesh=mesh,
        in_specs=placed,
        out_specs=(P(("grp", "ep", "tp"), None), P(("grp", "ep"), "tp", None, None)),
        check_vma=False,
    )
```
